256 devices in a mesh: sp: 32 (over z, x), tp: 8 (over y, core).
Axes of the slice: x: 4, y: 4, z: 8, core: 2. Of those that a mesh axis runs over, the one named last changes fastest.
Arguments:
- activations: bfloat16 [16384, 1024], P(('sp', 'tp')), may hold values from -8 to 8, as said below
- input_gain: float32 [1024], replicated, may hold values from 0.5 to 1.5
- query_weight: bfloat16 [1024, 1024], P(None, 'tp'), may hold values from -0.1875 to 0.1875
- key_weight: bfloat16 [1024, 1024], P(None, 'tp'), may hold values from -0.375 to 0.375
- value_weight: bfloat16 [1024, 1024], P(None, 'tp'), may hold values from -0.1875 to 0.1875
- stop_offset: float32 [16], P('tp'), may hold values from -16 to 0, as said below
- output_weight: bfloat16 [1024, 1024], P('tp'), may hold values from -0.1875 to 0.1875
- output_gain: float32 [1024], replicated, may hold values from 0.5 to 1.5
Outputs:
- layer_out: bfloat16 [16384, 1024], P(('sp', 'tp'))
The draws below stay inside these ranges and needn't reach their ends.
Inputs may be any that keep to these rules, and one draw needn't show every extreme that they name: activations are noise of about unit size plus a mean vector of about unit size shared by each aligned block of 512 rows and different between runs; each row as a whole may also be scaled by a factor between 0.25 and 2; the result is clipped to the range. `stop_offset`: each entry equals minus the natural logarithm of 16384, minus 2, plus the natural logarithm of 3, plus a number between 0 and 0.7.
All inputs are finite; a program needn't handle non-finite values.
Results may differ from the reference program's by a relative error of at most 0.015.
Values may be sent and summed in bfloat16 or wider, within the bound.
A program may use at most 128 MiB of HBM per device.

```python
import jax
import jax.numpy as jnp
from jax import lax

D = 1024
HEADS = 16
HEAD_DIM = 64
TOK_DEV = 512
TOKENS = 16384


def draw_activations(key, part):
    noise_key, mean_key, scale_key = jax.random.split(key, 3)
    blocks = TOKENS // TOK_DEV
    noise_part = jax.random.normal(noise_key, (blocks, TOK_DEV, D), jnp.float32)
    block_means = jax.random.normal(mean_key, (blocks, 1, D), jnp.float32)
    combined = noise_part + block_means
    return jnp.clip(combined, -8.0, 8.0).reshape(TOKENS, D).astype(jnp.bfloat16)


def draw_stop_offset(key, part):
    center = -jnp.log(jnp.float32(TOKENS)) - 2.0 + jnp.log(jnp.float32(3.0))
    return center + jax.random.uniform(key, (HEADS,), jnp.float32, 0.0, 0.7)


def steps_of(own_key, dims, cuts, least, top_value):
    loudness, own = 1.0, jax.random.fold_in(own_key, 6)
    for position, parts in cuts:
        draws = jnp.exp(jax.random.uniform(jax.random.fold_in(own, position), (parts,), jnp.float32, least / len(cuts), top_value / len(cuts)))
        loudness = loudness * jnp.repeat(draws, dims[position] // parts).reshape([-1 if axis == position else 1 for axis in range(len(dims))])
    return loudness


def centred(rng, dims, width, most, cuts=(), kind=jnp.bfloat16):
    level = steps_of(rng, dims, cuts, -0.22, 0.18) if cuts else 1.0
    drawn = jax.random.normal(rng, dims, jnp.float32) * width * level
    return jnp.minimum(jnp.maximum(drawn, -most), most).astype(kind)


def setup_inputs(seed: int = 0) -> dict:
    arg_keys = jax.random.split(jax.random.key(seed), 9)
    return {
        "activations": draw_activations(jax.random.fold_in(arg_keys[8], 71), 0),
        "input_gain": jnp.clip(1.0 + 0.1 * jax.random.normal(arg_keys[1], (D,), jnp.float32), 0.5, 1.5),
        "query_weight": centred(arg_keys[2], (D, HEADS * HEAD_DIM), D ** -0.5, 0.1875, ((1, 8),)),
        "key_weight": centred(arg_keys[3], (D, HEADS * HEAD_DIM), (D // 4) ** -0.5, 0.375, ((1, 8),)),
        "value_weight": centred(arg_keys[4], (D, HEADS * HEAD_DIM), D ** -0.5, 0.1875, ((1, 8),)),
        "stop_offset": draw_stop_offset(jax.random.fold_in(arg_keys[8], 71), 0),
        "output_weight": centred(arg_keys[6], (HEADS * HEAD_DIM, D), (HEADS * HEAD_DIM) ** -0.5, 0.1875, ((0, 8),)),
        "output_gain": jnp.clip(1.0 + 0.1 * jax.random.normal(arg_keys[7], (D,), jnp.float32), 0.5, 1.5),
    }


epsilon = 1e-06

def scaled_rows(row_block, row_gain):
    widened = row_block.astype(jnp.float32)
    spread = lax.optimization_barrier(jnp.mean(widened * widened, axis=-1, keepdims=True))
    return (widened * lax.rsqrt(spread + epsilon) * row_gain).astype(jnp.bfloat16)

def reference(activations, input_gain, query_weight, key_weight, value_weight, stop_offset, output_weight, output_gain):
    normed = scaled_rows(activations, input_gain)
    query_rows = jnp.dot(normed, query_weight, preferred_element_type=jnp.float32).astype(jnp.bfloat16)
    key_rows = jnp.dot(normed, key_weight, preferred_element_type=jnp.float32).astype(jnp.bfloat16)
    value_rows = jnp.dot(normed, value_weight, preferred_element_type=jnp.float32).astype(jnp.bfloat16)
    blocks = TOKENS // TOK_DEV
    query_blocks = query_rows.reshape(blocks, TOK_DEV, HEADS, HEAD_DIM)
    key_blocks = key_rows.reshape(blocks, TOK_DEV, HEADS, HEAD_DIM)
    value_blocks = value_rows.reshape(blocks, TOK_DEV, HEADS, HEAD_DIM)
    score_scale = HEAD_DIM ** (-0.5)
    offsets = stop_offset.astype(jnp.float32)

    def attend_block(query_index):
        queries = query_blocks[query_index].astype(jnp.float32)
        first_query = query_index * TOK_DEV

        def per_key(key_index):

            def compute(unused):
                key_here = key_blocks[key_index].astype(jnp.float32)
                value_here = value_blocks[key_index].astype(jnp.float32)
                scores = jnp.einsum('thd,shd->hts', queries, key_here, precision=lax.Precision.HIGHEST)
                scores = scores * score_scale + offsets[:, None, None]
                query_pos = first_query + jnp.arange(TOK_DEV, dtype=jnp.int32)
                key_pos = key_index * TOK_DEV + jnp.arange(TOK_DEV, dtype=jnp.int32)
                earlier = key_pos[None, :] < query_pos[:, None]
                log_keep = jnp.where(earlier[None], jax.nn.log_sigmoid(-scores), 0.0)
                within = lax.cumsum(log_keep, axis=2, reverse=True) - log_keep
                weights = jnp.where(earlier[None], jnp.exp(jax.nn.log_sigmoid(scores) + within), 0.0)
                weights = weights.astype(jnp.bfloat16).astype(jnp.float32)
                shard_part = jnp.einsum('hts,shd->thd', weights, value_here, precision=lax.Precision.HIGHEST)
                return (shard_part, lax.optimization_barrier(jnp.sum(log_keep, axis=2)))

            def skipped(unused):
                return (jnp.zeros((TOK_DEV, HEADS, HEAD_DIM), jnp.float32), jnp.zeros((HEADS, TOK_DEV), jnp.float32))
            return lax.cond(key_index <= query_index, compute, skipped, 0)
        block_parts, totals = lax.map(per_key, jnp.arange(blocks, dtype=jnp.int32))
        prefix_sums = jnp.cumsum(totals, axis=0)
        factors = jnp.exp(prefix_sums[-1:] - prefix_sums)
        combined = jnp.einsum('bht,bthd->thd', factors, block_parts, precision=lax.Precision.HIGHEST)
        return combined.astype(jnp.bfloat16)
    attended = lax.map(attend_block, jnp.arange(blocks, dtype=jnp.int32))
    attended = attended.reshape(TOKENS, HEADS * HEAD_DIM)
    projected = jnp.dot(attended, output_weight, preferred_element_type=jnp.float32)
    return scaled_rows(projected, output_gain)
```

```python
import functools

import jax
import jax.numpy as jnp
from jax import lax
from jax.experimental import pallas as pl
from jax.experimental.pallas import tpu as pltpu
from jax.sharding import PartitionSpec as P

epsilon = 1e-06
LANES = 128
SUB = 8
NT = (((1,), (1,)), ((), ()))


def scaled_rows(row_block, row_gain):
    widened = row_block.astype(jnp.float32)
    spread = jnp.mean(widened * widened, axis=-1, keepdims=True)
    return (widened * lax.rsqrt(spread + epsilon) * row_gain).astype(jnp.bfloat16)


def head_operands(raw, offset, h, half):
    lane = lax.broadcasted_iota(jnp.int32, raw.shape, 1)
    mine = (lane >= h * half) & (lane < (h + 1) * half)
    base = (1 - h) * half
    first = jnp.full(raw.shape, offset, jnp.float32)
    one = first.astype(jnp.bfloat16)
    rest = first - one.astype(jnp.float32)
    two = rest.astype(jnp.bfloat16)
    three = (rest - two.astype(jnp.float32)).astype(jnp.bfloat16)
    parts = jnp.where(lane == base, one, jnp.where(lane == base + 1, two, jnp.where(lane == base + 2, three, jnp.zeros_like(one))))
    return jnp.where(mine, raw, parts)


def key_operand(k, h, half):
    lane = lax.broadcasted_iota(jnp.int32, k.shape, 1)
    mine = (lane >= h * half) & (lane < (h + 1) * half)
    base = (1 - h) * half
    ones = jnp.where((lane >= base) & (lane < base + 3), jnp.ones_like(k), jnp.zeros_like(k))
    return jnp.where(mine, k, ones)


def suffix_products(total):
    row = lax.broadcasted_iota(jnp.int32, total.shape, 0)
    one = jnp.ones_like(total)

    def up(x, k):
        return jnp.where(row < SUB - k, pltpu.roll(x, SUB - k, 0), one)

    y = up(total, 1)
    y = y * up(y, 1)
    y = y * up(y, 2)
    return y * up(y, 4)


def tile_weights(halved, carry):
    keys, n = halved.shape
    steps = keys // SUB
    t = jnp.tanh(halved)
    take = 1.0 + t
    keep = 1.0 - t
    run = jnp.ones((SUB, n), jnp.float32)
    local = [None] * steps
    for v in reversed(range(steps)):
        local[v] = take[v * SUB : (v + 1) * SUB] * run
        run = run * keep[v * SUB : (v + 1) * SUB]
    total = run * (2.0 ** -steps)
    factor = suffix_products(total) * carry
    after = factor * total
    carry = jnp.broadcast_to(after[0:1], (SUB, n))
    return jnp.concatenate([x * factor for x in local], axis=0).astype(jnp.bfloat16), carry


def attention_kernel(off_ref, q_ref, kp_ref, vt_ref, out_ref, qh_ref, acc_ref, carry_ref):
    half = q_ref.shape[1] // 2
    block = q_ref.shape[0]
    me = lax.axis_index("sp")
    for h in range(2):
        qh_ref[h] = head_operands(q_ref[...], off_ref[h] * 0.5, h, half)
    acc_ref[...] = jnp.zeros_like(acc_ref)
    carry_ref[...] = jnp.ones_like(carry_ref)

    def tile(kb, h, diagonal):
        kh = key_operand(kp_ref[kb], h, half)
        halved = lax.dot_general(kh, qh_ref[h], NT, preferred_element_type=jnp.float32)
        if diagonal:
            row = lax.broadcasted_iota(jnp.int32, halved.shape, 0)
            query = lax.broadcasted_iota(jnp.int32, halved.shape, 1)
            key = lax.rem(row, SUB) * (block // SUB) + lax.div(row, SUB)
            halved = jnp.where(key < query, halved, -1e9)
        weights, carry_ref[h] = tile_weights(halved, carry_ref[h])
        acc_ref[h * half : (h + 1) * half] += jnp.dot(
            vt_ref[kb, h * half : (h + 1) * half], weights, preferred_element_type=jnp.float32
        )

    for h in range(2):
        tile(me, h, True)

    def body(i, c):
        for h in range(2):
            tile(me - 1 - i, h, False)
        return c

    lax.fori_loop(0, me, body, 0)
    out_ref[...] = jnp.transpose(acc_ref[...]).astype(out_ref.dtype)


def local(activations, input_gain, query_weight, key_weight, value_weight, stop_offset, output_weight, output_gain):
    normed = scaled_rows(activations, input_gain)
    whole = lax.all_gather(normed, "tp", axis=0, tiled=True)

    def proj(w):
        return jnp.dot(whole, w, preferred_element_type=jnp.float32).astype(jnp.bfloat16)

    q = proj(query_weight) * jnp.bfloat16(0.0625)
    k, v = proj(key_weight), proj(value_weight)
    block, width = q.shape
    steps = block // SUB
    perm = lambda a: a.reshape(SUB, steps, width).transpose(1, 0, 2).reshape(block, width)
    scale = jnp.repeat(2.0 ** -(steps - jnp.arange(steps, dtype=jnp.float32)), SUB)
    kp = perm(k)
    vt = (perm(v) * scale[:, None].astype(jnp.bfloat16)).T
    kp = lax.all_gather(kp, "sp", axis=0, tiled=False)
    vt = lax.all_gather(vt, "sp", axis=0, tiled=False)
    attended = pl.pallas_call(
        attention_kernel,
        out_shape=jax.ShapeDtypeStruct((block, width), jnp.bfloat16),
        in_specs=[pl.BlockSpec(memory_space=pltpu.SMEM)] + [pl.BlockSpec(memory_space=pltpu.VMEM)] * 3,
        out_specs=pl.BlockSpec(memory_space=pltpu.VMEM),
        scratch_shapes=[
            pltpu.VMEM((2, block, width), jnp.bfloat16),
            pltpu.VMEM((width, block), jnp.float32),
            pltpu.VMEM((2, SUB, block), jnp.float32),
        ],
        compiler_params=pltpu.CompilerParams(vmem_limit_bytes=48 * 1024 * 1024),
    )(stop_offset, q, kp, vt)
    out = jnp.dot(attended, output_weight, preferred_element_type=jnp.float32).astype(jnp.bfloat16)
    summed = lax.psum_scatter(out, "tp", scatter_dimension=0, tiled=True).astype(jnp.float32)
    return scaled_rows(summed, output_gain)


def solution(mesh):
    in_specs = (P(("sp", "tp"), None), P(), P(None, "tp"), P(None, "tp"), P(None, "tp"), P("tp"), P("tp", None), P())
    return jax.shard_map(local, mesh=mesh, in_specs=in_specs, out_specs=P(("sp", "tp"), None), check_vma=False)
```

```python
import jax
import jax.numpy as jnp
from jax import lax
from jax.experimental import pallas as pl
from jax.experimental.pallas import tpu as pltpu
from jax.sharding import PartitionSpec as P

epsilon = 1e-06
LANES = 128
SUB = 8
NT = (((1,), (1,)), ((), ()))


def head_operands(raw, offset, h, half):
    lane = lax.broadcasted_iota(jnp.int32, raw.shape, 1)
    mine = (lane >= h * half) & (lane < (h + 1) * half)
    base = (1 - h) * half
    first = jnp.full(raw.shape, offset, jnp.float32)
    one = first.astype(jnp.bfloat16)
    rest = first - one.astype(jnp.float32)
    two = rest.astype(jnp.bfloat16)
    three = (rest - two.astype(jnp.float32)).astype(jnp.bfloat16)
    parts = jnp.where(lane == base, one, jnp.where(lane == base + 1, two, jnp.where(lane == base + 2, three, jnp.zeros_like(one))))
    return jnp.where(mine, raw, parts)


def key_operand(k, h, half):
    lane = lax.broadcasted_iota(jnp.int32, k.shape, 1)
    mine = (lane >= h * half) & (lane < (h + 1) * half)
    base = (1 - h) * half
    ones = jnp.where((lane >= base) & (lane < base + 3), jnp.ones_like(k), jnp.zeros_like(k))
    return jnp.where(mine, k, ones)


def suffix_products(total):
    row = lax.broadcasted_iota(jnp.int32, total.shape, 0)
    one = jnp.ones_like(total)

    def up(x, k):
        return jnp.where(row < SUB - k, pltpu.roll(x, SUB - k, 0), one)

    y = up(total, 1)
    y = y * up(y, 1)
    y = y * up(y, 2)
    return y * up(y, 4)


def tile_weights(halved, carry):
    keys, n = halved.shape
    steps = keys // SUB
    t = jnp.tanh(halved)
    take = 1.0 + t
    keep = 1.0 - t
    run = jnp.ones((SUB, n), jnp.float32)
    local = [None] * steps
    for v in reversed(range(steps)):
        local[v] = take[v * SUB : (v + 1) * SUB] * run
        run = run * keep[v * SUB : (v + 1) * SUB]
    total = run * (2.0 ** -steps)
    factor = suffix_products(total) * carry
    after = factor * total
    carry = jnp.broadcast_to(after[0:1], (SUB, n))
    return jnp.concatenate([x * factor for x in local], axis=0).astype(jnp.bfloat16), carry


MESH = pl.DeviceIdType.MESH
XN, ZN, YN = 4, 8, 4
ORDER = (1, 7, 2, 6, 3, 5, 4)


def pick(values, index):
    out = jnp.int32(values[0])
    for position, value in enumerate(values[1:], 1):
        out = jnp.where(index == position, jnp.int32(value), out)
    return out


def layer_kernel(
    off_ref, x_ref, gain_ref, wq_ref, wk_ref, wv_ref, wo_ref, ogain_ref, out_ref,
    xall, pm, pms, wvt, kbuf, vbuf, qbuf, qh, acc, carry, own_acc, own_keep, send_out, send_keep,
    ret_out, ret_keep, att, att_in, wo_all,
    x_send, x_recv, k_send, k_recv, v_send, v_recv, q_send, q_recv, ro_send, ro_recv, rk_send, rk_recv,
    a_send, a_recv, w_send, w_recv,
):
    sp, tp = lax.axis_index("sp"), lax.axis_index("tp")
    z, x = lax.div(sp, XN), lax.rem(sp, XN)
    y, c = lax.div(tp, 2), lax.rem(tp, 2)
    partner = (sp, y * 2 + 1 - c)
    rows, model = x_ref.shape
    chunks = YN * 2
    block = rows * chunks
    width = wq_ref.shape[1]
    half = width // 2
    steps = block // SUB

    def at_tp(other):
        return (sp, other)

    def at_x(other):
        return (z * XN + other, tp)

    def at_z(other):
        return (other * XN + x, tp)

    def copy(src, dst, ss, rs, device):
        return pltpu.make_async_remote_copy(src_ref=src, dst_ref=dst, send_sem=ss, recv_sem=rs, device_id=device, device_id_type=MESH)

    barrier = pltpu.get_barrier_semaphore()
    peers = [at_tp(lax.rem(tp + d, chunks)) for d in range(1, chunks)]
    peers += [at_x(lax.rem(x + d, XN)) for d in range(1, XN)]
    peers += [at_z(lax.rem(z + d, ZN)) for d in range(1, ZN)]
    for peer in peers:
        pl.semaphore_signal(barrier, inc=1, device_id=peer, device_id_type=MESH)
    wide = x_ref[...].astype(jnp.float32)
    spread = jnp.mean(wide * wide, axis=-1, keepdims=True)
    xall[tp] = (wide * lax.rsqrt(spread + epsilon) * gain_ref[...]).astype(jnp.bfloat16)
    pl.semaphore_wait(barrier, len(peers))

    def x_copy(chunk, slot, device):
        return copy(xall.at[chunk], xall.at[chunk], x_send.at[slot], x_recv.at[chunk], device)

    for d in (1, 3, 2):
        x_copy(tp, d - 1, at_tp(lax.rem(y + d, YN) * 2 + c)).start()
    x_copy(tp, 3, partner).start()

    row = lax.broadcasted_iota(jnp.int32, (block, block), 0)
    col = lax.broadcasted_iota(jnp.int32, (block, block), 1)
    token_of_row = lax.rem(row, SUB) * steps + lax.div(row, SUB)
    pm[...] = jnp.where(col == token_of_row, 1.0, 0.0).astype(jnp.bfloat16)
    token_of_col = lax.rem(col, SUB) * steps + lax.div(col, SUB)
    power = jnp.exp2((lax.div(col[0:1], SUB) - steps).astype(jnp.float32))
    pms[...] = jnp.where(row == token_of_col, power, 0.0).astype(jnp.bfloat16)
    wvt[...] = jnp.transpose(wv_ref[...])

    for d in (1, 3, 2):
        chunk = lax.rem(y + d, YN) * 2 + c
        x_copy(chunk, d - 1, partner).wait_recv()
        x_copy(chunk, 3 + d, partner).start()
    x_copy(y * 2 + 1 - c, 3, partner).wait_recv()
    for d in (1, 3, 2):
        x_copy(lax.rem(y + d, YN) * 2 + 1 - c, 3, partner).wait_recv()

    def w_copy(slot, d):
        return copy(wo_ref, wo_all.at[slot], w_send.at[d - 1], w_recv.at[slot], at_tp(lax.rem(tp + d, chunks)))

    normed = xall[...].reshape(block, model)
    q = jnp.dot(normed, wq_ref[...], preferred_element_type=jnp.float32).astype(jnp.bfloat16)
    qbuf[z] = q * jnp.bfloat16(0.0625)

    def q_copy(d):
        return copy(qbuf.at[z], qbuf.at[z], q_send.at[d - 1], q_recv.at[z], at_z(z - d))

    k = jnp.dot(normed, wk_ref[...], preferred_element_type=jnp.float32).astype(jnp.bfloat16)
    kbuf[x] = jnp.dot(pm[...], k, preferred_element_type=jnp.float32).astype(jnp.bfloat16)
    vt = lax.dot_general(wvt[...], normed, NT, preferred_element_type=jnp.float32).astype(jnp.bfloat16)
    vbuf[x] = jnp.dot(vt, pms[...], preferred_element_type=jnp.float32).astype(jnp.bfloat16)

    def k_copy(slot, d):
        return copy(kbuf.at[slot], kbuf.at[slot], k_send.at[d - 1], k_recv.at[slot], at_x(lax.rem(x + d, XN)))

    def v_copy(slot, d):
        return copy(vbuf.at[slot], vbuf.at[slot], v_send.at[d - 1], v_recv.at[slot], at_x(lax.rem(x + d, XN)))

    for d in (1, 3, 2):
        k_copy(x, d).start()
        v_copy(x, d).start()
    for d in ORDER:
        @pl.when(z >= d)
        def _():
            q_copy(d).start()
    for d in range(1, chunks):
        w_copy(tp, d).start()

    def prepare(slot):
        for h in range(2):
            qh[h] = head_operands(qbuf[slot], off_ref[h] * 0.5, h, half)
        acc[...] = jnp.zeros_like(acc)
        carry[...] = jnp.ones_like(carry)

    def tile(kb, h, diagonal):
        kh = key_operand(kbuf[kb], h, half)
        halved = lax.dot_general(kh, qh[h], NT, preferred_element_type=jnp.float32)
        if diagonal:
            query = lax.broadcasted_iota(jnp.int32, halved.shape, 1)
            row = lax.broadcasted_iota(jnp.int32, halved.shape, 0)
            halved = jnp.where(lax.rem(row, SUB) * steps + lax.div(row, SUB) < query, halved, -1e9)
        weights, carry[h] = tile_weights(halved, carry[h])
        acc[h * half : (h + 1) * half] += jnp.dot(vbuf[kb, h * half : (h + 1) * half], weights, preferred_element_type=jnp.float32)

    def tiles_down_from(first):
        def step(i, s):
            for h in range(2):
                tile(first - i, h, False)
            return s

        lax.fori_loop(0, first + 1, step, 0)

    prepare(z)
    for h in range(2):
        tile(x, h, True)
    for d in range(1, XN):
        other = lax.rem(x + d, XN)
        k_copy(other, 1).wait_recv()
        v_copy(other, 1).wait_recv()
    tiles_down_from(x - 1)
    own_acc[...] = acc[...]
    for h in range(2):
        own_keep[h : h + 1] = carry[h, 0:1]

    def out_copy(s, z_to):
        return copy(send_out.at[s], ret_out.at[z], ro_send.at[s], ro_recv.at[z], at_z(z_to))

    def keep_copy(s, z_to):
        return copy(send_keep.at[s], ret_keep.at[z], rk_send.at[s], rk_recv.at[z], at_z(z_to))

    def later(s, t):
        source = z + pick(ORDER, s)

        @pl.when(source < ZN)
        def _():
            copy(qbuf.at[source], qbuf.at[source], q_send.at[0], q_recv.at[source], partner).wait_recv()
            prepare(source)
            tiles_down_from(jnp.int32(XN - 1))
            send_out[s] = acc[...].astype(jnp.bfloat16)
            for h in range(2):
                send_keep[s, h : h + 1] = carry[h, 0:1]
            out_copy(s, source).start()
            keep_copy(s, source).start()

        return t

    lax.fori_loop(0, ZN - 1, later, 0)

    acc[...] = jnp.zeros_like(acc)

    def earlier(source, t):
        copy(ret_out.at[source], ret_out.at[source], ro_send.at[0], ro_recv.at[source], partner).wait_recv()
        copy(ret_keep.at[source], ret_keep.at[source], rk_send.at[0], rk_recv.at[source], partner).wait_recv()
        for h in range(2):
            part = slice(h * half, (h + 1) * half)
            acc[part] = acc[part] * ret_keep[source, h : h + 1] + ret_out[source, part].astype(jnp.float32)
        return t

    lax.fori_loop(0, z, earlier, 0)
    for h in range(2):
        part = slice(h * half, (h + 1) * half)
        acc[part] = acc[part] * own_keep[h : h + 1] + own_acc[part]
    att[...] = jnp.transpose(acc[...]).astype(jnp.bfloat16).reshape(att.shape)

    def a_copy(d):
        other = lax.rem(tp + d, chunks)
        return copy(att.at[other], att_in.at[tp], a_send.at[d - 1], a_recv.at[tp], at_tp(other))

    for d in range(1, chunks):
        a_copy(d).start()
    total = jnp.dot(att[tp], wo_ref[...], preferred_element_type=jnp.float32)
    for d in range(1, chunks):
        other = lax.rem(tp + d, chunks)
        w_copy(other, d).wait_recv()
        copy(att_in.at[other], att_in.at[other], a_send.at[0], a_recv.at[other], partner).wait_recv()
        total = total + jnp.dot(att_in[other], wo_all[other], preferred_element_type=jnp.float32)
    spread = jnp.mean(total * total, axis=-1, keepdims=True)
    out_ref[...] = (total * lax.rsqrt(spread + epsilon) * ogain_ref[...]).astype(jnp.bfloat16)

    for slot in range(chunks - 1):
        x_copy(tp, slot, partner).wait_send()
    for d in range(1, XN):
        k_copy(x, d).wait_send()
        v_copy(x, d).wait_send()
    for d in ORDER:
        @pl.when(z >= d)
        def _():
            q_copy(d).wait_send()
    for d in range(1, chunks):
        w_copy(tp, d).wait_send()
        a_copy(d).wait_send()

    def sent(s, t):
        @pl.when(z + pick(ORDER, s) < ZN)
        def _():
            out_copy(s, z).wait_send()
            keep_copy(s, z).wait_send()

        return t

    lax.fori_loop(0, ZN - 1, sent, 0)


def local(activations, input_gain, query_weight, key_weight, value_weight, stop_offset, output_weight, output_gain):
    rows, model = activations.shape
    width = query_weight.shape[1]
    chunks = lax.axis_size("tp")
    block = rows * chunks
    bf, f32, dma = jnp.bfloat16, jnp.float32, pltpu.SemaphoreType.DMA
    vmem = pl.BlockSpec(memory_space=pltpu.VMEM)
    return pl.pallas_call(
        layer_kernel,
        out_shape=jax.ShapeDtypeStruct((rows, model), bf),
        in_specs=[pl.BlockSpec(memory_space=pltpu.SMEM)] + [vmem] * 7,
        out_specs=vmem,
        scratch_shapes=[
            pltpu.VMEM((chunks, rows, model), bf),
            pltpu.VMEM((block, block), bf),
            pltpu.VMEM((block, block), bf),
            pltpu.VMEM((width, model), bf),
            pltpu.VMEM((XN, block, width), bf),
            pltpu.VMEM((XN, width, block), bf),
            pltpu.VMEM((ZN, block, width), bf),
            pltpu.VMEM((2, block, width), bf),
            pltpu.VMEM((width, block), f32),
            pltpu.VMEM((2, SUB, block), f32),
            pltpu.VMEM((width, block), f32),
            pltpu.VMEM((2, block), f32),
            pltpu.VMEM((ZN - 1, width, block), bf),
            pltpu.VMEM((ZN - 1, 2, block), f32),
            pltpu.VMEM((ZN, width, block), bf),
            pltpu.VMEM((ZN, 2, block), f32),
            pltpu.VMEM((chunks, rows, width), bf),
            pltpu.VMEM((chunks, rows, width), bf),
            pltpu.VMEM((chunks, width, model), bf),
            dma((7,)), dma((chunks,)),
            dma((3,)), dma((XN,)), dma((3,)), dma((XN,)),
            dma((7,)), dma((ZN,)),
            dma((7,)), dma((ZN,)), dma((7,)), dma((ZN,)),
            dma((7,)), dma((chunks,)), dma((7,)), dma((chunks,)),
        ],
        compiler_params=pltpu.CompilerParams(collective_id=0, has_side_effects=True, vmem_limit_bytes=56 * 1024 * 1024),
    )(stop_offset, activations, input_gain[None], query_weight, key_weight, value_weight, output_weight, output_gain[None])


def solution(mesh):
    in_specs = (P(("sp", "tp"), None), P(), P(None, "tp"), P(None, "tp"), P(None, "tp"), P("tp"), P("tp", None), P())
    return jax.shard_map(local, mesh=mesh, in_specs=in_specs, out_specs=P(("sp", "tp"), None), check_vma=False)
```

```python
import jax
import jax.numpy as jnp
from jax import lax
from jax.experimental import pallas as pl
from jax.experimental.pallas import tpu as pltpu
from jax.sharding import PartitionSpec as P

epsilon = 1e-06
SUB = 8
NT = (((1,), (1,)), ((), ()))
MESH = pl.DeviceIdType.MESH
XN, ZN, YN = 4, 8, 4
LAST = ZN - 1
Q_ORDER = (7, 6, 1, 5, 2, 4, 3)


def suffix_products(total):
    row = lax.broadcasted_iota(jnp.int32, total.shape, 0)

    def up(a, k):
        return jnp.where(row < SUB - k, pltpu.roll(a, SUB - k, 0), 1.0)

    y = up(total, 1)
    y = y * up(y, 1)
    y = y * up(y, 2)
    return y * up(y, 4)


def tile_weights(halved, carry, w_ref):
    keys, n = halved.shape
    steps = keys // SUB
    run = jnp.ones((SUB, n), jnp.float32)
    local = []
    for v in range(steps):
        part = run * jnp.tanh(halved[v * SUB : (v + 1) * SUB])
        local.append(run + part)
        run = run - part
    total = run * (2.0**-steps)
    factor = suffix_products(total) * carry
    for u in range(steps // 2):
        pair = jnp.concatenate([local[2 * u] * factor, local[2 * u + 1] * factor], axis=0)
        w_ref[2 * SUB * u : 2 * SUB * (u + 1)] = pair.astype(jnp.bfloat16)
    return jnp.broadcast_to((factor * total)[0:1], (SUB, n))


def layer_kernel(
    off_ref, x_ref, gain_ref, wq_ref, wk_ref, wv_ref, wo_ref, ogain_ref, out_ref,
    xall, wt, pk, pv_, qmine, kmate, vmate, qbuf, kt, vt, kop, qop, wa, wb, wc, wd, acc, carry,
    send_out, send_keep, ret_out, ret_keep, att, att_in, wo_all,
    x_send, x_recv, xh_recv, m_send, k_send, k_recv, v_send, v_recv, q_send, q_recv,
    ro_send, ro_recv, rk_send, rk_recv, a_send, a_recv, w_send, w_recv,
):
    sp, tp = lax.axis_index("sp"), lax.axis_index("tp")
    z, x = lax.div(sp, XN), lax.rem(sp, XN)
    y, c = lax.div(tp, 2), lax.rem(tp, 2)
    mate = LAST - z
    head = lax.div(z, ZN // 2)
    other = 1 - head
    partner = (sp, y * 2 + 1 - c)
    rows, model = x_ref.shape
    chunks = YN * 2
    block = rows * chunks
    width = wq_ref.shape[1]
    half = width // 2
    steps = block // SUB
    bf, f32 = jnp.bfloat16, jnp.float32

    def at_tp(o):
        return (sp, o)

    def at_x(o):
        return (z * XN + o, tp)

    def at_z(o):
        return (o * XN + x, tp)

    def copy(src, dst, ss, rs, device):
        return pltpu.make_async_remote_copy(src_ref=src, dst_ref=dst, send_sem=ss, recv_sem=rs, device_id=device, device_id_type=MESH)

    def along_y(d):
        return lax.rem(y + d, YN)

    def along_x(d):
        return lax.rem(x + d, XN)

    barrier = pltpu.get_barrier_semaphore()
    peers = [at_tp(lax.rem(tp + d, chunks)) for d in range(1, chunks)]
    peers += [at_x(along_x(1)), at_x(along_x(XN - 1))]
    peers += [at_z(lax.rem(z + d, ZN)) for d in range(1, ZN)]
    for peer in peers:
        pl.semaphore_signal(barrier, inc=1, device_id=peer, device_id_type=MESH)
    wide = x_ref[...].astype(f32)
    spread = jnp.mean(wide * wide, axis=-1, keepdims=True)
    xall[tp] = (wide * lax.rsqrt(spread + epsilon) * gain_ref[...]).astype(bf).reshape(xall.shape[1:])
    pl.semaphore_wait(barrier, len(peers))

    def x_full(chunk, slot, device):
        return copy(xall.at[chunk], xall.at[chunk], x_send.at[slot], x_recv.at[chunk], device)

    def x_half(chunk, part, slot, side, device):
        return copy(xall.at[chunk, part], xall.at[chunk, part], x_send.at[slot], xh_recv.at[side, part], device)

    def same(d):
        return along_y(d) * 2 + c

    def across(d):
        return along_y(d) * 2 + 1 - c

    x_full(tp, 0, at_tp(same(1))).start()
    x_full(tp, 1, at_tp(same(3))).start()
    x_full(tp, 2, partner).start()

    row = lax.broadcasted_iota(jnp.int32, (block, block), 0)
    col = lax.broadcasted_iota(jnp.int32, (1, block), 1)
    step_of = lax.div(col, SUB)
    hit = row == lax.rem(col, SUB) * steps + (steps - 1) - step_of
    pk[...] = jnp.where(hit, 1.0, 0.0).astype(bf)
    pv_[...] = jnp.where(hit, jnp.exp2(-(step_of + 1).astype(f32)), 0.0).astype(bf)
    wt[0] = jnp.transpose(wq_ref[...])
    wt[1] = jnp.transpose(wk_ref[...])
    wt[2] = jnp.transpose(wv_ref[...])
    low = lax.broadcasted_iota(jnp.int32, (half, block), 0)
    first = jnp.full((half, block), off_ref[head] * 0.5, f32)
    one = first.astype(bf)
    rest = first - one.astype(f32)
    two = rest.astype(bf)
    three = (rest - two.astype(f32)).astype(bf)
    qop[half:] = jnp.where(low == 0, one, jnp.where(low == 1, two, jnp.where(low == 2, three, jnp.zeros_like(one))))
    ones = jnp.where(low < 3, 1.0, 0.0).astype(bf)

    x_full(same(3), 0, partner).wait_recv()
    x_half(same(3), 0, 3, 0, at_tp(same(1))).start()
    x_full(same(3), 4, partner).start()
    x_full(same(1), 0, partner).wait_recv()
    x_half(same(1), 1, 5, 0, at_tp(same(3))).start()
    x_full(same(1), 6, partner).start()
    for part in range(2):
        x_half(same(2), part, 0, 0, partner).wait_recv()
        x_half(same(2), part, 7 + part, 1, partner).start()
    for d in (0, 1, 3):
        x_full(across(d), 0, partner).wait_recv()
    for part in range(2):
        x_half(across(2), part, 0, 1, partner).wait_recv()

    normed = xall[...].reshape(block, model)
    projected = lax.dot_general(wt[...].reshape(3 * width, model), normed, NT, preferred_element_type=f32).astype(bf)
    q_all = projected[0:width] * bf(0.0625)
    k_all = jnp.dot(projected[width : 2 * width], pk[...], preferred_element_type=f32).astype(bf)
    v_all = jnp.dot(projected[2 * width :], pv_[...], preferred_element_type=f32).astype(bf)
    qmine[...] = q_all.reshape(qmine.shape)
    k_two = k_all.reshape(2, half, block)
    v_two = v_all.reshape(2, half, block)
    upper = head == 1
    kt[head, x] = jnp.where(upper, k_two[1], k_two[0])
    vt[head, x] = jnp.where(upper, v_two[1], v_two[0])
    kmate[...] = jnp.where(upper, k_two[0], k_two[1])
    vmate[...] = jnp.where(upper, v_two[0], v_two[1])

    def k_copy(slab, chunk, slot, device):
        return copy(kt.at[slab, chunk], kt.at[slab, chunk], k_send.at[slab, slot], k_recv.at[slab, chunk], device)

    def v_copy(slab, chunk, slot, device):
        return copy(vt.at[slab, chunk], vt.at[slab, chunk], v_send.at[slab, slot], v_recv.at[slab, chunk], device)

    def mate_copies():
        return (
            copy(kmate, kt.at[head, x], m_send.at[0], k_recv.at[head, x], at_z(mate)),
            copy(vmate, vt.at[head, x], m_send.at[1], v_recv.at[head, x], at_z(mate)),
        )

    def spread_block(slab):
        for slot, d in ((0, 1), (1, XN - 1)):
            k_copy(slab, x, slot, at_x(along_x(d))).start()
            v_copy(slab, x, slot, at_x(along_x(d))).start()

    def pass_on(slab):
        left, right = along_x(XN - 1), along_x(1)
        k_copy(slab, left, 0, partner).wait_recv()
        k_copy(slab, left, 2, at_x(right)).start()
        v_copy(slab, right, 0, partner).wait_recv()
        v_copy(slab, right, 2, at_x(left)).start()
        v_copy(slab, left, 0, partner).wait_recv()
        k_copy(slab, right, 0, partner).wait_recv()

    def opposite(slab):
        far = along_x(2)
        k_copy(slab, far, 0, partner).wait_recv()
        v_copy(slab, far, 0, partner).wait_recv()

    def key_rows(slab, chunk):
        kop[slab, chunk] = jnp.transpose(jnp.concatenate([kt[slab, chunk], ones], axis=0))

    for sent in mate_copies():
        sent.start()
    spread_block(head)

    def target(d):
        return lax.rem(z + d, ZN)

    def reaches(d):
        return jnp.minimum(target(d), LAST - target(d)) <= z

    def q_copy(d):
        return copy(qmine.at[lax.div(target(d), ZN // 2)], qbuf.at[z], q_send.at[d - 1], q_recv.at[z], at_z(target(d)))

    for d in Q_ORDER:
        @pl.when(reaches(d))
        def _():
            q_copy(d).start()

    def w_copy(slot, d):
        return copy(wo_ref, wo_all.at[slot], w_send.at[d - 1], w_recv.at[slot], at_tp(lax.rem(tp + d, chunks)))

    for d in range(1, chunks):
        w_copy(tp, d).start()

    def q_arrived(source):
        copy(qbuf.at[source], qbuf.at[source], q_send.at[0], q_recv.at[source], partner).wait_recv()

    def scores(slab, kb):
        return jnp.dot(kop[slab, kb], qop[...], preferred_element_type=f32)

    def values(slab, kb, w_ref):
        return jnp.dot(vt[slab, kb], w_ref[...], preferred_element_type=f32)

    def out_copy(slab, source):
        index = jnp.where(slab == head, z, mate)
        return (
            copy(send_out.at[slab, source], ret_out.at[index, head], ro_send.at[slab, source], ro_recv.at[index, head], at_z(source)),
            copy(send_keep.at[slab, source], ret_keep.at[index, head], rk_send.at[slab, source], rk_recv.at[index, head], at_z(source)),
        )

    def deliver(slab, source, part, keep):
        @pl.when(source == z)
        def _():
            index = jnp.where(slab == head, z, mate)
            ret_out[index, head] = part.astype(bf)
            ret_keep[index, head] = keep[0:1]

        @pl.when(source != z)
        def _():
            send_out[slab, source] = part.astype(bf)
            send_keep[slab, source] = keep[0:1]
            for sent in out_copy(slab, source):
                sent.start()

    def full_set(slab, source):
        qop[0:half] = qbuf[source]
        keep = jnp.ones((SUB, block), f32)
        keep = tile_weights(scores(slab, 3), keep, wa)
        keep = tile_weights(scores(slab, 2), keep, wb)
        part = values(slab, 3, wa)
        keep = tile_weights(scores(slab, 1), keep, wc)
        part = part + values(slab, 2, wb)
        keep = tile_weights(scores(slab, 0), keep, wd)
        part = part + values(slab, 1, wc)
        part = part + values(slab, 0, wd)
        deliver(slab, source, part, keep)

    def diagonal_tile(slab):
        halved = scores(slab, x)
        r = lax.broadcasted_iota(jnp.int32, halved.shape, 0)
        query = lax.broadcasted_iota(jnp.int32, halved.shape, 1)
        key = lax.rem(r, SUB) * steps + (steps - 1) - lax.div(r, SUB)
        halved = jnp.where(key < query, halved, -1e9)
        carry[...] = tile_weights(halved, jnp.ones((SUB, block), f32), wa)
        acc[0:half] = values(slab, x, wa)

    def below_diagonal(slab, source):
        def step(i, t):
            kb = x - 1 - i
            carry[...] = tile_weights(scores(slab, kb), carry[...], wa)
            acc[0:half] += values(slab, kb, wa)
            return t

        lax.fori_loop(0, x, step, 0)
        deliver(slab, source, acc[0:half], carry[...])

    qbuf[z] = qmine[head]
    qop[0:half] = qmine[head]
    key_rows(head, x)
    diagonal_tile(head)
    pass_on(head)
    k_copy(other, x, 0, partner).wait_recv()
    v_copy(other, x, 0, partner).wait_recv()
    spread_block(other)
    opposite(head)
    for d in range(1, XN):
        key_rows(head, along_x(d))
    below_diagonal(head, z)

    own_jobs = LAST - z

    def job(n, t):
        @pl.when(n == jnp.minimum(2, own_jobs))
        def _():
            pass_on(other)

        @pl.when(n == own_jobs)
        def _():
            opposite(other)
            for d in range(XN):
                key_rows(other, along_x(d))

        @pl.when(n < LAST)
        def _():
            mine = n < own_jobs
            slab = jnp.where(mine, head, other)
            source = jnp.where(mine, z + 1 + n, n + 1)

            @pl.when(mine | (source < z))
            def _():
                q_arrived(source)

            full_set(slab, source)

        return t

    lax.fori_loop(0, ZN, job, 0)

    @pl.when(upper)
    def _():
        q_arrived(mate)

    qop[0:half] = qbuf[mate]
    diagonal_tile(other)
    below_diagonal(other, mate)

    acc[...] = jnp.zeros_like(acc)

    def gather(slab, t):
        for h in range(2):
            low_z = jnp.minimum(slab, LAST - slab)
            provider = low_z if h == 0 else LAST - low_z

            @pl.when(provider != z)
            def _():
                copy(ret_out.at[slab, h], ret_out.at[slab, h], ro_send.at[0, 0], ro_recv.at[slab, h], partner).wait_recv()
                copy(ret_keep.at[slab, h], ret_keep.at[slab, h], rk_send.at[0, 0], rk_recv.at[slab, h], partner).wait_recv()

            span = slice(h * half, (h + 1) * half)
            acc[span] = acc[span] * ret_keep[slab, h] + ret_out[slab, h].astype(f32)
        return t

    lax.fori_loop(0, z + 1, gather, 0)
    att[...] = jnp.transpose(acc[...]).astype(bf).reshape(att.shape)

    def a_copy(d):
        o = lax.rem(tp + d, chunks)
        return copy(att.at[o], att_in.at[tp], a_send.at[d - 1], a_recv.at[tp], at_tp(o))

    for d in range(1, chunks):
        a_copy(d).start()
    total = jnp.dot(att[tp], wo_ref[...], preferred_element_type=f32)
    for d in range(1, chunks):
        o = lax.rem(tp + d, chunks)
        w_copy(o, d).wait_recv()
        copy(att_in.at[o], att_in.at[o], a_send.at[0], a_recv.at[o], partner).wait_recv()
        total = total + jnp.dot(att_in[o], wo_all[o], preferred_element_type=f32)
    spread = jnp.mean(total * total, axis=-1, keepdims=True)
    out_ref[...] = (total * lax.rsqrt(spread + epsilon) * ogain_ref[...]).astype(bf)

    for slot in (0, 1, 2, 4, 6):
        x_full(tp, slot, partner).wait_send()
    for slot in (3, 5, 7, 8):
        x_half(tp, 0, slot, 0, partner).wait_send()
    for sent in mate_copies():
        sent.wait_send()
    for slab in range(2):
        for slot in range(3):
            k_copy(slab, x, slot, partner).wait_send()
            v_copy(slab, x, slot, partner).wait_send()
    for d in Q_ORDER:
        @pl.when(reaches(d))
        def _():
            q_copy(d).wait_send()
    for d in range(1, chunks):
        w_copy(tp, d).wait_send()
        a_copy(d).wait_send()

    def drained(source, t):
        @pl.when((source >= z) & (source != z))
        def _():
            for sent in out_copy(head, source):
                sent.wait_send()

        @pl.when((source >= mate) & (source != z))
        def _():
            for sent in out_copy(other, source):
                sent.wait_send()

        return t

    lax.fori_loop(0, ZN, drained, 0)


def local(activations, input_gain, query_weight, key_weight, value_weight, stop_offset, output_weight, output_gain):
    rows, model = activations.shape
    width = query_weight.shape[1]
    half = width // 2
    chunks = lax.axis_size("tp")
    block = rows * chunks
    bf, f32, dma = jnp.bfloat16, jnp.float32, pltpu.SemaphoreType.DMA
    vmem = pl.BlockSpec(memory_space=pltpu.VMEM)
    return pl.pallas_call(
        layer_kernel,
        out_shape=jax.ShapeDtypeStruct((rows, model), bf),
        in_specs=[pl.BlockSpec(memory_space=pltpu.SMEM)] + [vmem] * 7,
        out_specs=vmem,
        scratch_shapes=[
            pltpu.VMEM((chunks, 2, rows // 2, model), bf),
            pltpu.VMEM((3, width, model), bf),
            pltpu.VMEM((block, block), bf),
            pltpu.VMEM((block, block), bf),
            pltpu.VMEM((2, half, block), bf),
            pltpu.VMEM((half, block), bf),
            pltpu.VMEM((half, block), bf),
            pltpu.VMEM((ZN, half, block), bf),
            pltpu.VMEM((2, XN, half, block), bf),
            pltpu.VMEM((2, XN, half, block), bf),
            pltpu.VMEM((2, XN, block, width), bf),
            pltpu.VMEM((width, block), bf),
            *[pltpu.VMEM((block, block), bf)] * 4,
            pltpu.VMEM((width, block), f32),
            pltpu.VMEM((SUB, block), f32),
            pltpu.VMEM((2, ZN, half, block), bf),
            pltpu.VMEM((2, ZN, 1, block), f32),
            pltpu.VMEM((ZN, 2, half, block), bf),
            pltpu.VMEM((ZN, 2, 1, block), f32),
            pltpu.VMEM((chunks, rows, width), bf),
            pltpu.VMEM((chunks, rows, width), bf),
            pltpu.VMEM((chunks, width, model), bf),
            dma((9,)), dma((chunks,)), dma((2, 2)), dma((2,)),
            dma((2, 3)), dma((2, XN)), dma((2, 3)), dma((2, XN)),
            dma((7,)), dma((ZN,)),
            dma((2, ZN)), dma((ZN, 2)), dma((2, ZN)), dma((ZN, 2)),
            dma((7,)), dma((chunks,)), dma((7,)), dma((chunks,)),
        ],
        compiler_params=pltpu.CompilerParams(collective_id=0, has_side_effects=True, vmem_limit_bytes=56 * 1024 * 1024),
    )(stop_offset, activations, input_gain[None], query_weight, key_weight, value_weight, output_weight, output_gain[None])


def solution(mesh):
    in_specs = (P(("sp", "tp"), None), P(), P(None, "tp"), P(None, "tp"), P(None, "tp"), P("tp"), P("tp", None), P())
    return jax.shard_map(local, mesh=mesh, in_specs=in_specs, out_specs=P(("sp", "tp"), None), check_vma=False)
```

```python
import jax
import jax.numpy as jnp
from jax import lax
from jax.experimental import pallas as pl
from jax.experimental.pallas import tpu as pltpu
from jax.sharding import PartitionSpec as P

epsilon = 1e-06
SUB = 8
NT = (((1,), (1,)), ((), ()))
MESH = pl.DeviceIdType.MESH
XN, ZN, YN = 4, 8, 4
LAST = ZN - 1
Q_ORDER = (7, 6, 1, 5, 2, 4, 3)


def suffix_products(total):
    row = lax.broadcasted_iota(jnp.int32, total.shape, 0)

    def up(a, k):
        return jnp.where(row < SUB - k, pltpu.roll(a, SUB - k, 0), 1.0)

    y = up(total, 1)
    y = y * up(y, 1)
    y = y * up(y, 2)
    return y * up(y, 4)


def tile_weights(halved, carry, w_ref):
    keys, n = halved.shape
    steps = keys // SUB
    run = jnp.ones((SUB, n), jnp.float32)
    local = []
    for v in range(steps):
        part = run * jnp.tanh(halved[v * SUB : (v + 1) * SUB])
        local.append(run + part)
        run = run - part
    total = run * (2.0**-steps)
    factor = suffix_products(total) * carry
    for u in range(steps // 2):
        pair = jnp.concatenate([local[2 * u] * factor, local[2 * u + 1] * factor], axis=0)
        w_ref[2 * SUB * u : 2 * SUB * (u + 1)] = pair.astype(jnp.bfloat16)
    return jnp.broadcast_to((factor * total)[0:1], (SUB, n))


def layer_kernel(
    off_ref, x_ref, gain_ref, wq_ref, wk_ref, wv_ref, wo_ref, ogain_ref, out_ref,
    xall, wt, pk, pv_, qmine, kmate, vmate, qbuf, kt, vt, kop, qop, wa, wb, wc, wd, acc, carry,
    send_out, send_keep, ret_out, ret_keep, att, att_in, wo_all,
    x_send, x_recv, m_send, k_send, k_recv, v_send, v_recv, q_send, q_recv,
    ro_send, ro_recv, rk_send, rk_recv, a_send, a_recv, w_send, w_recv,
):
    sp, tp = lax.axis_index("sp"), lax.axis_index("tp")
    z, x = lax.div(sp, XN), lax.rem(sp, XN)
    y, c = lax.div(tp, 2), lax.rem(tp, 2)
    mate = LAST - z
    head = lax.div(z, ZN // 2)
    other = 1 - head
    partner = (sp, y * 2 + 1 - c)
    rows, model = x_ref.shape
    chunks = YN * 2
    block = rows * chunks
    width = wq_ref.shape[1]
    half = width // 2
    steps = block // SUB
    bf, f32 = jnp.bfloat16, jnp.float32

    def at_tp(o):
        return (sp, o)

    def at_x(o):
        return (z * XN + o, tp)

    def at_z(o):
        return (o * XN + x, tp)

    def copy(src, dst, ss, rs, device):
        return pltpu.make_async_remote_copy(src_ref=src, dst_ref=dst, send_sem=ss, recv_sem=rs, device_id=device, device_id_type=MESH)

    def along_y(d):
        return lax.rem(y + d, YN)

    def along_x(d):
        return lax.rem(x + d, XN)

    barrier = pltpu.get_barrier_semaphore()
    peers = [at_tp(lax.rem(tp + d, chunks)) for d in range(1, chunks)]
    peers += [at_x(along_x(1)), at_x(along_x(XN - 1))]
    peers += [at_z(lax.rem(z + d, ZN)) for d in range(1, ZN)]
    for peer in peers:
        pl.semaphore_signal(barrier, inc=1, device_id=peer, device_id_type=MESH)
    wide = x_ref[...].astype(f32)
    spread = jnp.mean(wide * wide, axis=-1, keepdims=True)
    xall[tp] = (wide * lax.rsqrt(spread + epsilon) * gain_ref[...]).astype(bf).reshape(xall.shape[1:])
    pl.semaphore_wait(barrier, len(peers))

    def same(d):
        return along_y(d) * 2 + c

    def across(d):
        return along_y(d) * 2 + 1 - c

    class TpGather:
        def __init__(self, buf, send, recv):
            self.buf, self.send, self.recv = buf, send, recv

        def part(self, chunk, h, slot, device):
            piece = self.buf.at[chunk, h]
            return copy(piece, piece, self.send.at[slot], self.recv.at[chunk, h], device)

        def begin(self):
            for slot, (h, device) in enumerate(((0, same(1)), (1, same(3)), (1, same(1)), (0, same(3)))):
                self.part(tp, h, slot, at_tp(device)).start()
            for h in range(2):
                self.part(tp, h, 4 + h, partner).start()

        def take(self, chunk, h, slot):
            self.part(chunk, h, 0, partner).wait_recv()
            if slot is not None:
                self.part(chunk, h, slot, partner).start()

        def relay(self):
            self.take(same(3), 0, 6)
            self.part(same(3), 0, 12, at_tp(same(1))).start()
            self.take(same(1), 1, 7)
            self.part(same(1), 1, 13, at_tp(same(3))).start()
            self.take(same(3), 1, 8)
            self.take(same(1), 0, 9)

        def relay_far(self):
            self.take(same(2), 0, 10)
            self.take(same(2), 1, 11)

        def complete(self):
            for d in (0, 1, 3, 2):
                for h in range(2):
                    self.take(across(d), h, None)

        def drain(self):
            for slot in range(14):
                self.part(tp, 0, slot, partner).wait_send()

    x_gather = TpGather(xall, x_send, x_recv)
    w_gather = TpGather(wo_all, w_send, w_recv)
    x_gather.begin()
    wo_all[tp] = wo_ref[...].reshape(wo_all.shape[1:])

    row = lax.broadcasted_iota(jnp.int32, (block, block), 0)
    col = lax.broadcasted_iota(jnp.int32, (1, block), 1)
    step_of = lax.div(col, SUB)
    hit = row == lax.rem(col, SUB) * steps + (steps - 1) - step_of
    pk[...] = jnp.where(hit, 1.0, 0.0).astype(bf)
    pv_[...] = jnp.where(hit, jnp.exp2(-(step_of + 1).astype(f32)), 0.0).astype(bf)
    wt[0] = jnp.transpose(wq_ref[...])
    wt[1] = jnp.transpose(wk_ref[...])
    wt[2] = jnp.transpose(wv_ref[...])
    low = lax.broadcasted_iota(jnp.int32, (half, block), 0)
    first = jnp.full((half, block), off_ref[head] * 0.5, f32)
    one = first.astype(bf)
    rest = first - one.astype(f32)
    two = rest.astype(bf)
    three = (rest - two.astype(f32)).astype(bf)
    qop[half:] = jnp.where(low == 0, one, jnp.where(low == 1, two, jnp.where(low == 2, three, jnp.zeros_like(one))))
    ones = jnp.where(low < 3, 1.0, 0.0).astype(bf)

    x_gather.relay()
    x_gather.relay_far()
    x_gather.complete()

    normed = xall[...].reshape(block, model)
    projected = lax.dot_general(wt[...].reshape(3 * width, model), normed, NT, preferred_element_type=f32).astype(bf)
    q_all = projected[0:width] * bf(0.0625)
    k_all = jnp.dot(projected[width : 2 * width], pk[...], preferred_element_type=f32).astype(bf)
    v_all = jnp.dot(projected[2 * width :], pv_[...], preferred_element_type=f32).astype(bf)
    qmine[...] = q_all.reshape(qmine.shape)
    k_two = k_all.reshape(2, half, block)
    v_two = v_all.reshape(2, half, block)
    upper = head == 1
    kt[head, x] = jnp.where(upper, k_two[1], k_two[0])
    vt[head, x] = jnp.where(upper, v_two[1], v_two[0])
    kmate[...] = jnp.where(upper, k_two[0], k_two[1])
    vmate[...] = jnp.where(upper, v_two[0], v_two[1])

    def k_copy(slab, chunk, slot, device):
        return copy(kt.at[slab, chunk], kt.at[slab, chunk], k_send.at[slab, slot], k_recv.at[slab, chunk], device)

    def v_copy(slab, chunk, slot, device):
        return copy(vt.at[slab, chunk], vt.at[slab, chunk], v_send.at[slab, slot], v_recv.at[slab, chunk], device)

    def mate_copies():
        return (
            copy(kmate, kt.at[head, x], m_send.at[0], k_recv.at[head, x], at_z(mate)),
            copy(vmate, vt.at[head, x], m_send.at[1], v_recv.at[head, x], at_z(mate)),
        )

    def spread_keys(slab):
        for slot, d in ((0, 1), (1, XN - 1)):
            k_copy(slab, x, slot, at_x(along_x(d))).start()

    def spread_values(slab):
        for slot, d in ((0, XN - 1), (1, 1)):
            v_copy(slab, x, slot, at_x(along_x(d))).start()

    left, right = along_x(XN - 1), along_x(1)

    def pass_on(slab):
        k_copy(slab, left, 0, partner).wait_recv()
        k_copy(slab, left, 2, at_x(right)).start()
        v_copy(slab, right, 0, partner).wait_recv()
        v_copy(slab, right, 2, at_x(left)).start()

    def beside(slab):
        v_copy(slab, left, 0, partner).wait_recv()
        k_copy(slab, right, 0, partner).wait_recv()

    def opposite(slab):
        far = along_x(2)
        k_copy(slab, far, 0, partner).wait_recv()
        v_copy(slab, far, 0, partner).wait_recv()

    def key_rows(slab, chunk):
        kop[slab, chunk] = jnp.transpose(jnp.concatenate([kt[slab, chunk], ones], axis=0))

    for sent in mate_copies():
        sent.start()
    spread_keys(head)
    spread_values(head)

    def target(d):
        return lax.rem(z + d, ZN)

    def reaches(d):
        return jnp.minimum(target(d), LAST - target(d)) <= z

    def q_copy(d):
        return copy(qmine.at[lax.div(target(d), ZN // 2)], qbuf.at[z], q_send.at[d - 1], q_recv.at[z], at_z(target(d)))

    for d in Q_ORDER:
        @pl.when(reaches(d))
        def _():
            q_copy(d).start()

    w_gather.begin()

    def q_arrived(source):
        copy(qbuf.at[source], qbuf.at[source], q_send.at[0], q_recv.at[source], partner).wait_recv()

    def scores(slab, kb):
        return jnp.dot(kop[slab, kb], qop[...], preferred_element_type=f32)

    def values(slab, kb, w_ref):
        return jnp.dot(vt[slab, kb], w_ref[...], preferred_element_type=f32)

    centre = (z == ZN // 2 - 1) | (z == ZN // 2)

    def joined(source):
        return centre & (source >= ZN // 2)

    def slab_index(slab, source):
        return jnp.where(joined(source), ZN // 2, jnp.where(slab == head, z, mate))

    def out_copy(slab, source):
        index = slab_index(slab, source)
        return (
            copy(send_out.at[slab, source], ret_out.at[index, head], ro_send.at[slab, source], ro_recv.at[index, head], at_z(source)),
            copy(send_keep.at[slab, source], ret_keep.at[index, head], rk_send.at[slab, source], rk_recv.at[index, head], at_z(source)),
        )

    def deliver(slab, source, part, keep):
        acc[0:half] = part
        carry[...] = keep

        @pl.when(joined(source) & (slab == other))
        def _():
            before, kept = send_out[head, source].astype(f32), send_keep[head, source]
            now = acc[0:half]
            first, second = jnp.where(upper, before, now), jnp.where(upper, now, before)
            acc[0:half] = first + jnp.where(upper, kept, carry[0:1]) * second
            carry[0:1] = carry[0:1] * kept

        waits = joined(source) & (slab == head)

        @pl.when((source == z) & jnp.logical_not(waits))
        def _():
            index = slab_index(slab, source)
            ret_out[index, head] = acc[0:half].astype(bf)
            ret_keep[index, head] = carry[0:1]

        @pl.when((source != z) | waits)
        def _():
            send_out[slab, source] = acc[0:half].astype(bf)
            send_keep[slab, source] = carry[0:1]

        @pl.when((source != z) & jnp.logical_not(waits))
        def _():
            for sent in out_copy(slab, source):
                sent.start()

    def full_set(slab, source):
        qop[0:half] = qbuf[source]
        keep = jnp.ones((SUB, block), f32)
        keep = tile_weights(scores(slab, 3), keep, wa)
        keep = tile_weights(scores(slab, 2), keep, wb)
        part = values(slab, 3, wa)
        keep = tile_weights(scores(slab, 1), keep, wc)
        part = part + values(slab, 2, wb)
        keep = tile_weights(scores(slab, 0), keep, wd)
        part = part + values(slab, 1, wc)
        part = part + values(slab, 0, wd)
        deliver(slab, source, part, keep)

    def diagonal_tile(slab):
        halved = scores(slab, x)
        r = lax.broadcasted_iota(jnp.int32, halved.shape, 0)
        query = lax.broadcasted_iota(jnp.int32, halved.shape, 1)
        key = lax.rem(r, SUB) * steps + (steps - 1) - lax.div(r, SUB)
        halved = jnp.where(key < query, halved, -1e9)
        carry[...] = tile_weights(halved, jnp.ones((SUB, block), f32), wa)
        acc[0:half] = values(slab, x, wa)

    def below_diagonal(slab, source):
        def step(i, t):
            kb = x - 1 - i
            carry[...] = tile_weights(scores(slab, kb), carry[...], wa)
            acc[0:half] += values(slab, kb, wa)
            return t

        lax.fori_loop(0, x, step, 0)
        deliver(slab, source, acc[0:half], carry[...])

    qbuf[z] = qmine[head]
    qop[0:half] = qmine[head]
    key_rows(head, x)
    diagonal_tile(head)
    pass_on(head)
    k_copy(other, x, 0, partner).wait_recv()
    spread_keys(other)
    v_copy(other, x, 0, partner).wait_recv()
    spread_values(other)
    beside(head)
    opposite(head)
    w_gather.relay()
    for d in range(1, XN):
        key_rows(head, along_x(d))
    below_diagonal(head, z)

    own_jobs = LAST - z

    def job(n, t):
        @pl.when(n == jnp.minimum(2, own_jobs))
        def _():
            pass_on(other)

        @pl.when(n == 3)
        def _():
            w_gather.relay_far()

        @pl.when(n == own_jobs)
        def _():
            beside(other)
            opposite(other)
            for d in range(XN):
                key_rows(other, along_x(d))

        @pl.when(n < LAST)
        def _():
            mine = n < own_jobs
            slab = jnp.where(mine, head, other)
            source = jnp.where(mine, z + 1 + n, n + 1)

            @pl.when(mine | (source < z))
            def _():
                q_arrived(source)

            full_set(slab, source)

        return t

    lax.fori_loop(0, ZN, job, 0)

    @pl.when(upper)
    def _():
        q_arrived(mate)

    qop[0:half] = qbuf[mate]
    diagonal_tile(other)
    below_diagonal(other, mate)

    acc[...] = jnp.zeros_like(acc)

    def gather(slab, t):
        for h in range(2):
            low_z = jnp.minimum(slab, LAST - slab)
            provider = low_z if h == 0 else LAST - low_z
            held = (slab != ZN // 2 - 1) | (z < ZN // 2)

            @pl.when(held & (provider != z))
            def _():
                copy(ret_out.at[slab, h], ret_out.at[slab, h], ro_send.at[0, 0], ro_recv.at[slab, h], partner).wait_recv()
                copy(ret_keep.at[slab, h], ret_keep.at[slab, h], rk_send.at[0, 0], rk_recv.at[slab, h], partner).wait_recv()

            @pl.when(held)
            def _():
                span = slice(h * half, (h + 1) * half)
                acc[span] = acc[span] * ret_keep[slab, h] + ret_out[slab, h].astype(f32)

        return t

    lax.fori_loop(0, z + 1, gather, 0)
    att[...] = jnp.transpose(acc[...]).astype(bf).reshape(att.shape)

    def a_copy(d):
        o = lax.rem(tp + d, chunks)
        return copy(att.at[o], att_in.at[tp], a_send.at[d - 1], a_recv.at[tp], at_tp(o))

    for d in range(1, chunks):
        a_copy(d).start()
    total = jnp.dot(att[tp], wo_ref[...], preferred_element_type=f32)
    w_gather.complete()
    for d in range(1, chunks):
        o = lax.rem(tp + d, chunks)
        copy(att_in.at[o], att_in.at[o], a_send.at[0], a_recv.at[o], partner).wait_recv()
        total = total + jnp.dot(att_in[o], wo_all[o].reshape(width, model), preferred_element_type=f32)
    spread = jnp.mean(total * total, axis=-1, keepdims=True)
    out_ref[...] = (total * lax.rsqrt(spread + epsilon) * ogain_ref[...]).astype(bf)

    x_gather.drain()
    w_gather.drain()
    for sent in mate_copies():
        sent.wait_send()
    for slab in range(2):
        for slot in range(3):
            k_copy(slab, x, slot, partner).wait_send()
            v_copy(slab, x, slot, partner).wait_send()
    for d in Q_ORDER:
        @pl.when(reaches(d))
        def _():
            q_copy(d).wait_send()
    for d in range(1, chunks):
        a_copy(d).wait_send()

    def drained(source, t):
        @pl.when((source > z) & jnp.logical_not(joined(source)))
        def _():
            for sent in out_copy(head, source):
                sent.wait_send()

        @pl.when((source >= mate) & (source != z))
        def _():
            for sent in out_copy(other, source):
                sent.wait_send()

        return t

    lax.fori_loop(0, ZN, drained, 0)


def local(activations, input_gain, query_weight, key_weight, value_weight, stop_offset, output_weight, output_gain):
    rows, model = activations.shape
    width = query_weight.shape[1]
    half = width // 2
    chunks = lax.axis_size("tp")
    block = rows * chunks
    bf, f32, dma = jnp.bfloat16, jnp.float32, pltpu.SemaphoreType.DMA
    vmem = pl.BlockSpec(memory_space=pltpu.VMEM)
    return pl.pallas_call(
        layer_kernel,
        out_shape=jax.ShapeDtypeStruct((rows, model), bf),
        in_specs=[pl.BlockSpec(memory_space=pltpu.SMEM)] + [vmem] * 7,
        out_specs=vmem,
        scratch_shapes=[
            pltpu.VMEM((chunks, 2, rows // 2, model), bf),
            pltpu.VMEM((3, width, model), bf),
            pltpu.VMEM((block, block), bf),
            pltpu.VMEM((block, block), bf),
            pltpu.VMEM((2, half, block), bf),
            pltpu.VMEM((half, block), bf),
            pltpu.VMEM((half, block), bf),
            pltpu.VMEM((ZN, half, block), bf),
            pltpu.VMEM((2, XN, half, block), bf),
            pltpu.VMEM((2, XN, half, block), bf),
            pltpu.VMEM((2, XN, block, width), bf),
            pltpu.VMEM((width, block), bf),
            *[pltpu.VMEM((block, block), bf)] * 4,
            pltpu.VMEM((width, block), f32),
            pltpu.VMEM((SUB, block), f32),
            pltpu.VMEM((2, ZN, half, block), bf),
            pltpu.VMEM((2, ZN, 1, block), f32),
            pltpu.VMEM((ZN, 2, half, block), bf),
            pltpu.VMEM((ZN, 2, 1, block), f32),
            pltpu.VMEM((chunks, rows, width), bf),
            pltpu.VMEM((chunks, rows, width), bf),
            pltpu.VMEM((chunks, 2, width // 2, model), bf),
            dma((14,)), dma((chunks, 2)), dma((2,)),
            dma((2, 3)), dma((2, XN)), dma((2, 3)), dma((2, XN)),
            dma((7,)), dma((ZN,)),
            dma((2, ZN)), dma((ZN, 2)), dma((2, ZN)), dma((ZN, 2)),
            dma((7,)), dma((chunks,)), dma((14,)), dma((chunks, 2)),
        ],
        compiler_params=pltpu.CompilerParams(collective_id=0, has_side_effects=True, vmem_limit_bytes=56 * 1024 * 1024),
    )(stop_offset, activations, input_gain[None], query_weight, key_weight, value_weight, output_weight, output_gain[None])


def solution(mesh):
    in_specs = (P(("sp", "tp"), None), P(), P(None, "tp"), P(None, "tp"), P(None, "tp"), P("tp"), P("tp", None), P())
    return jax.shard_map(local, mesh=mesh, in_specs=in_specs, out_specs=P(("sp", "tp"), None), check_vma=False)
```

```python
import jax
import jax.numpy as jnp
from jax import lax
from jax.experimental import pallas as pl
from jax.experimental.pallas import tpu as pltpu
from jax.sharding import PartitionSpec as P

epsilon = 1e-06
SUB = 8
NT = (((1,), (1,)), ((), ()))
MESH = pl.DeviceIdType.MESH
XN, ZN, YN = 4, 8, 4
LAST = ZN - 1
Q_ORDER = (7, 6, 1, 5, 2, 4, 3)
OWN_ORDER = (1, 7, 2, 6, 3, 5, 4)
MATE_ORDER = (6, 2, 5, 3, 4, 7, 1, 0)


def pick(values, index):
    out = jnp.int32(values[0])
    for position, value in enumerate(values[1:], 1):
        out = jnp.where(index == position, jnp.int32(value), out)
    return out


def suffix_products(total):
    row = lax.broadcasted_iota(jnp.int32, total.shape, 0)

    def up(a, k):
        return jnp.where(row < SUB - k, pltpu.roll(a, SUB - k, 0), 1.0)

    y = up(total, 1)
    y = y * up(y, 1)
    y = y * up(y, 2)
    return y * up(y, 4)


def tile_weights(halved, carry, w_ref):
    keys, n = halved.shape
    steps = keys // SUB
    run = jnp.ones((SUB, n), jnp.float32)
    local = []
    for v in range(steps):
        part = run * jnp.tanh(halved[v * SUB : (v + 1) * SUB])
        local.append(run + part)
        run = run - part
    total = run * (2.0**-steps)
    factor = suffix_products(total) * carry
    for u in range(steps // 2):
        pair = jnp.concatenate([local[2 * u] * factor, local[2 * u + 1] * factor], axis=0)
        w_ref[2 * SUB * u : 2 * SUB * (u + 1)] = pair.astype(jnp.bfloat16)
    return jnp.broadcast_to((factor * total)[0:1], (SUB, n))


def layer_kernel(
    off_ref, x_hbm, gain_hbm, wq_hbm, wk_hbm, wv_hbm, wo_hbm, ogain_hbm, out_ref,
    x_ref, gain_ref, wq_ref, wk_ref, wv_ref, ogain_ref, in_sem, xall, wt, pk, pv_, qmine, kmate, vmate, qbuf, kt, vt, kop, qop, wa, wb, wc, wd, acc, carry,
    send_out, send_keep, ret_out, ret_keep, att, att_in, wo_all,
    x_send, x_recv, m_send, k_send, k_recv, v_send, v_recv, q_send, q_recv,
    ro_send, ro_recv, rk_send, rk_recv, a_send, a_recv, w_send, w_recv,
):
    sp, tp = lax.axis_index("sp"), lax.axis_index("tp")
    z, x = lax.div(sp, XN), lax.rem(sp, XN)
    y, c = lax.div(tp, 2), lax.rem(tp, 2)
    mate = LAST - z
    head = lax.div(z, ZN // 2)
    other = 1 - head
    partner = (sp, y * 2 + 1 - c)
    rows, model = x_hbm.shape
    chunks = YN * 2
    block = rows * chunks
    width = wq_hbm.shape[1]
    half = width // 2
    steps = block // SUB
    bf, f32 = jnp.bfloat16, jnp.float32

    def at_tp(o):
        return (sp, o)

    def at_x(o):
        return (z * XN + o, tp)

    def at_z(o):
        return (o * XN + x, tp)

    def copy(src, dst, ss, rs, device):
        return pltpu.make_async_remote_copy(src_ref=src, dst_ref=dst, send_sem=ss, recv_sem=rs, device_id=device, device_id_type=MESH)

    def along_y(d):
        return lax.rem(y + d, YN)

    def along_x(d):
        return lax.rem(x + d, XN)

    barrier = pltpu.get_barrier_semaphore()
    peers = [at_tp(lax.rem(tp + d, chunks)) for d in range(1, chunks)]
    peers += [at_x(along_x(1)), at_x(along_x(XN - 1))]
    peers += [at_z(lax.rem(z + d, ZN)) for d in range(1, ZN)]
    for peer in peers:
        pl.semaphore_signal(barrier, inc=1, device_id=peer, device_id_type=MESH)
    weights_in = [
        pltpu.make_async_copy(src, dst, in_sem.at[n])
        for n, (src, dst) in enumerate(
            (
                (x_hbm, x_ref), (gain_hbm, gain_ref), (wq_hbm, wq_ref), (wk_hbm, wk_ref), (wv_hbm, wv_ref),
                (wo_hbm.at[0 : width // 2], wo_all.at[tp, 0]), (wo_hbm.at[width // 2 :], wo_all.at[tp, 1]), (ogain_hbm, ogain_ref),
            )
        )
    ]
    for piece in weights_in:
        piece.start()
    weights_in[0].wait()
    weights_in[1].wait()
    wide = x_ref[...].astype(f32)
    spread = jnp.mean(wide * wide, axis=-1, keepdims=True)
    xall[tp] = (wide * lax.rsqrt(spread + epsilon) * gain_ref[...]).astype(bf).reshape(xall.shape[1:])
    pl.semaphore_wait(barrier, len(peers))

    def same(d):
        return along_y(d) * 2 + c

    def across(d):
        return along_y(d) * 2 + 1 - c

    class TpGather:
        def __init__(self, buf, send, recv):
            self.buf, self.send, self.recv = buf, send, recv

        def part(self, chunk, h, slot, device):
            piece = self.buf.at[chunk, h]
            return copy(piece, piece, self.send.at[slot], self.recv.at[chunk, h], device)

        def begin(self):
            for slot, (h, device) in enumerate(((0, same(1)), (1, same(3)), (1, same(1)), (0, same(3)))):
                self.part(tp, h, slot, at_tp(device)).start()
            for h in range(2):
                self.part(tp, h, 4 + h, partner).start()

        def take(self, chunk, h, slot):
            self.part(chunk, h, 0, partner).wait_recv()
            if slot is not None:
                self.part(chunk, h, slot, partner).start()

        def relay(self):
            self.take(same(3), 0, 6)
            self.part(same(3), 0, 12, at_tp(same(1))).start()
            self.take(same(1), 1, 7)
            self.part(same(1), 1, 13, at_tp(same(3))).start()
            self.take(same(3), 1, 8)
            self.take(same(1), 0, 9)

        def relay_far(self):
            self.take(same(2), 0, 10)
            self.take(same(2), 1, 11)

        def complete(self):
            for d in (0, 1, 3, 2):
                for h in range(2):
                    self.take(across(d), h, None)

        def drain(self):
            for slot in range(14):
                self.part(tp, 0, slot, partner).wait_send()

    x_gather = TpGather(xall, x_send, x_recv)
    w_gather = TpGather(wo_all, w_send, w_recv)
    x_gather.begin()
    for piece in weights_in[2:]:
        piece.wait()

    row = lax.broadcasted_iota(jnp.int32, (block, block), 0)
    col = lax.broadcasted_iota(jnp.int32, (1, block), 1)
    step_of = lax.div(col, SUB)
    hit = row == lax.rem(col, SUB) * steps + (steps - 1) - step_of
    pk[...] = jnp.where(hit, 1.0, 0.0).astype(bf)
    pv_[...] = jnp.where(hit, jnp.exp2(-(step_of + 1).astype(f32)), 0.0).astype(bf)
    wt[0] = jnp.transpose(wq_ref[...])
    wt[1] = jnp.transpose(wk_ref[...])
    wt[2] = jnp.transpose(wv_ref[...])
    low = lax.broadcasted_iota(jnp.int32, (half, block), 0)
    first = jnp.full((half, block), off_ref[head] * 0.5, f32)
    one = first.astype(bf)
    rest = first - one.astype(f32)
    two = rest.astype(bf)
    three = (rest - two.astype(f32)).astype(bf)
    qop[half:] = jnp.where(low == 0, one, jnp.where(low == 1, two, jnp.where(low == 2, three, jnp.zeros_like(one))))
    ones = jnp.where(low < 3, 1.0, 0.0).astype(bf)

    x_gather.relay()
    x_gather.relay_far()
    x_gather.complete()

    normed = xall[...].reshape(block, model)
    projected = lax.dot_general(wt[...].reshape(3 * width, model), normed, NT, preferred_element_type=f32).astype(bf)
    q_all = projected[0:width] * bf(0.0625)
    k_all = jnp.dot(projected[width : 2 * width], pk[...], preferred_element_type=f32).astype(bf)
    v_all = jnp.dot(projected[2 * width :], pv_[...], preferred_element_type=f32).astype(bf)
    qmine[...] = q_all.reshape(qmine.shape)
    k_two = k_all.reshape(2, half, block)
    v_two = v_all.reshape(2, half, block)
    upper = head == 1
    kt[head, x] = jnp.where(upper, k_two[1], k_two[0])
    vt[head, x] = jnp.where(upper, v_two[1], v_two[0])
    kmate[...] = jnp.where(upper, k_two[0], k_two[1])
    vmate[...] = jnp.where(upper, v_two[0], v_two[1])

    def k_copy(slab, chunk, slot, device):
        return copy(kt.at[slab, chunk], kt.at[slab, chunk], k_send.at[slab, slot], k_recv.at[slab, chunk], device)

    def v_copy(slab, chunk, slot, device):
        return copy(vt.at[slab, chunk], vt.at[slab, chunk], v_send.at[slab, slot], v_recv.at[slab, chunk], device)

    def mate_copies():
        return (
            copy(kmate, kt.at[head, x], m_send.at[0], k_recv.at[head, x], at_z(mate)),
            copy(vmate, vt.at[head, x], m_send.at[1], v_recv.at[head, x], at_z(mate)),
        )

    def spread_keys(slab):
        for slot, d in ((0, 1), (1, XN - 1)):
            k_copy(slab, x, slot, at_x(along_x(d))).start()

    def spread_values(slab):
        for slot, d in ((0, XN - 1), (1, 1)):
            v_copy(slab, x, slot, at_x(along_x(d))).start()

    left, right = along_x(XN - 1), along_x(1)

    def pass_on(slab):
        k_copy(slab, left, 0, partner).wait_recv()
        k_copy(slab, left, 2, at_x(right)).start()
        v_copy(slab, right, 0, partner).wait_recv()
        v_copy(slab, right, 2, at_x(left)).start()

    def beside(slab):
        v_copy(slab, left, 0, partner).wait_recv()
        k_copy(slab, right, 0, partner).wait_recv()

    def opposite(slab):
        far = along_x(2)
        k_copy(slab, far, 0, partner).wait_recv()
        v_copy(slab, far, 0, partner).wait_recv()

    def key_rows(slab, chunk):
        kop[slab, chunk] = jnp.transpose(jnp.concatenate([kt[slab, chunk], ones], axis=0))

    for sent in mate_copies():
        sent.start()
    spread_keys(head)
    spread_values(head)

    def target(d):
        return lax.rem(z + d, ZN)

    def reaches(d):
        return jnp.minimum(target(d), LAST - target(d)) <= z

    def q_copy(d):
        return copy(qmine.at[lax.div(target(d), ZN // 2)], qbuf.at[z], q_send.at[d - 1], q_recv.at[z], at_z(target(d)))

    for d in Q_ORDER:
        @pl.when(reaches(d))
        def _():
            q_copy(d).start()

    w_gather.begin()

    def q_arrived(source):
        copy(qbuf.at[source], qbuf.at[source], q_send.at[0], q_recv.at[source], partner).wait_recv()

    def scores(slab, kb):
        return jnp.dot(kop[slab, kb], qop[...], preferred_element_type=f32)

    def values(slab, kb, w_ref):
        return jnp.dot(vt[slab, kb], w_ref[...], preferred_element_type=f32)

    centre = (z == ZN // 2 - 1) | (z == ZN // 2)

    def joined(source):
        return centre & (source >= ZN // 2)

    def slab_index(slab, source):
        return jnp.where(joined(source), ZN // 2, jnp.where(slab == head, z, mate))

    def out_copy(slab, source):
        index = slab_index(slab, source)
        return (
            copy(send_out.at[slab, source], ret_out.at[index, head], ro_send.at[slab, source], ro_recv.at[index, head], at_z(source)),
            copy(send_keep.at[slab, source], ret_keep.at[index, head], rk_send.at[slab, source], rk_recv.at[index, head], at_z(source)),
        )

    def deliver(slab, source, part, keep):
        acc[0:half] = part
        carry[...] = keep

        @pl.when(joined(source) & (slab == other))
        def _():
            before, kept = send_out[head, source].astype(f32), send_keep[head, source]
            now = acc[0:half]
            first, second = jnp.where(upper, before, now), jnp.where(upper, now, before)
            acc[0:half] = first + jnp.where(upper, kept, carry[0:1]) * second
            carry[0:1] = carry[0:1] * kept

        waits = joined(source) & (slab == head)

        @pl.when((source == z) & jnp.logical_not(waits))
        def _():
            index = slab_index(slab, source)
            ret_out[index, head] = acc[0:half].astype(bf)
            ret_keep[index, head] = carry[0:1]

        @pl.when((source != z) | waits)
        def _():
            send_out[slab, source] = acc[0:half].astype(bf)
            send_keep[slab, source] = carry[0:1]

        @pl.when((source != z) & jnp.logical_not(waits))
        def _():
            for sent in out_copy(slab, source):
                sent.start()

    def full_set(slab, source):
        qop[0:half] = qbuf[source]
        keep = jnp.ones((SUB, block), f32)
        keep = tile_weights(scores(slab, 3), keep, wa)
        keep = tile_weights(scores(slab, 2), keep, wb)
        part = values(slab, 3, wa)
        keep = tile_weights(scores(slab, 1), keep, wc)
        part = part + values(slab, 2, wb)
        keep = tile_weights(scores(slab, 0), keep, wd)
        part = part + values(slab, 1, wc)
        part = part + values(slab, 0, wd)
        deliver(slab, source, part, keep)

    def diagonal_tile(slab):
        halved = scores(slab, x)
        r = lax.broadcasted_iota(jnp.int32, halved.shape, 0)
        query = lax.broadcasted_iota(jnp.int32, halved.shape, 1)
        key = lax.rem(r, SUB) * steps + (steps - 1) - lax.div(r, SUB)
        halved = jnp.where(key < query, halved, -1e9)
        carry[...] = tile_weights(halved, jnp.ones((SUB, block), f32), wa)
        acc[0:half] = values(slab, x, wa)

    def below_diagonal(slab, source):
        def step(i, t):
            kb = x - 1 - i
            carry[...] = tile_weights(scores(slab, kb), carry[...], wa)
            acc[0:half] += values(slab, kb, wa)
            return t

        lax.fori_loop(0, x, step, 0)
        deliver(slab, source, acc[0:half], carry[...])

    qbuf[z] = qmine[head]
    qop[0:half] = qmine[head]
    key_rows(head, x)
    pass_on(head)
    k_copy(other, x, 0, partner).wait_recv()
    spread_keys(other)
    v_copy(other, x, 0, partner).wait_recv()
    spread_values(other)
    beside(head)
    opposite(head)
    diagonal_tile(head)
    for d in range(1, XN):
        key_rows(head, along_x(d))
    w_gather.relay()
    below_diagonal(head, z)

    def job(n, t):
        @pl.when(n == 2)
        def _():
            pass_on(other)

        @pl.when(n == 5)
        def _():
            w_gather.relay_far()

        @pl.when(n == LAST)
        def _():
            beside(other)
            opposite(other)
            for d in range(XN):
                key_rows(other, along_x(d))

        mine = n < LAST
        slab = jnp.where(mine, head, other)
        source = jnp.where(mine, z + pick(OWN_ORDER, n), lax.rem(z + pick(MATE_ORDER, n - LAST), ZN))

        @pl.when((source < ZN) & (mine | (source > mate)))
        def _():
            @pl.when(mine | (source < z))
            def _():
                q_arrived(source)

            full_set(slab, source)

        return t

    lax.fori_loop(0, LAST + ZN, job, 0)

    @pl.when(upper)
    def _():
        q_arrived(mate)

    qop[0:half] = qbuf[mate]
    diagonal_tile(other)
    below_diagonal(other, mate)

    acc[...] = jnp.zeros_like(acc)

    def gather(slab, t):
        for h in range(2):
            low_z = jnp.minimum(slab, LAST - slab)
            provider = low_z if h == 0 else LAST - low_z
            held = (slab != ZN // 2 - 1) | (z < ZN // 2)

            @pl.when(held & (provider != z))
            def _():
                copy(ret_out.at[slab, h], ret_out.at[slab, h], ro_send.at[0, 0], ro_recv.at[slab, h], partner).wait_recv()
                copy(ret_keep.at[slab, h], ret_keep.at[slab, h], rk_send.at[0, 0], rk_recv.at[slab, h], partner).wait_recv()

            @pl.when(held)
            def _():
                span = slice(h * half, (h + 1) * half)
                acc[span] = acc[span] * ret_keep[slab, h] + ret_out[slab, h].astype(f32)

        return t

    lax.fori_loop(0, z + 1, gather, 0)
    att[...] = jnp.transpose(acc[...]).astype(bf).reshape(att.shape)

    def lanes(core):
        return pl.ds(pl.multiple_of(core * width, width), width)

    def a_copy(d):
        o = lax.rem(tp + d, chunks)
        return copy(att.at[o], att_in.at[y, :, lanes(c)], a_send.at[d - 1], a_recv.at[tp], at_tp(o))

    for d in range(1, chunks):
        a_copy(d).start()
    att_in[y, :, lanes(c)] = att[tp]
    w_gather.complete()
    total = jnp.zeros((rows, model), f32)
    for d in (0, 1, 3, 2):
        pair = along_y(d)
        for o in (pair * 2 + 1 - c,) if d == 0 else (pair * 2 + c, pair * 2 + 1 - c):
            slot = att_in.at[pair, :, lanes(lax.rem(o, 2))]
            copy(slot, slot, a_send.at[0], a_recv.at[o], partner).wait_recv()
        both = wo_all[pl.ds(pair * 2, 2)].reshape(2 * width, model)
        total = total + jnp.dot(att_in[pair], both, preferred_element_type=f32)
    spread = jnp.mean(total * total, axis=-1, keepdims=True)
    out_ref[...] = (total * lax.rsqrt(spread + epsilon) * ogain_ref[...]).astype(bf)

    x_gather.drain()
    w_gather.drain()
    for sent in mate_copies():
        sent.wait_send()
    for slab in range(2):
        for slot in range(3):
            k_copy(slab, x, slot, partner).wait_send()
            v_copy(slab, x, slot, partner).wait_send()
    for d in Q_ORDER:
        @pl.when(reaches(d))
        def _():
            q_copy(d).wait_send()
    for d in range(1, chunks):
        a_copy(d).wait_send()

    def drained(source, t):
        @pl.when((source > z) & jnp.logical_not(joined(source)))
        def _():
            for sent in out_copy(head, source):
                sent.wait_send()

        @pl.when((source >= mate) & (source != z))
        def _():
            for sent in out_copy(other, source):
                sent.wait_send()

        return t

    lax.fori_loop(0, ZN, drained, 0)


def local(activations, input_gain, query_weight, key_weight, value_weight, stop_offset, output_weight, output_gain):
    rows, model = activations.shape
    width = query_weight.shape[1]
    half = width // 2
    chunks = lax.axis_size("tp")
    block = rows * chunks
    bf, f32, dma = jnp.bfloat16, jnp.float32, pltpu.SemaphoreType.DMA
    vmem = pl.BlockSpec(memory_space=pltpu.VMEM)
    return pl.pallas_call(
        layer_kernel,
        out_shape=jax.ShapeDtypeStruct((rows, model), bf),
        in_specs=[pl.BlockSpec(memory_space=pltpu.SMEM)] + [pl.BlockSpec(memory_space=pl.ANY)] * 7,
        out_specs=vmem,
        scratch_shapes=[
            pltpu.VMEM((rows, model), bf),
            pltpu.VMEM((1, model), f32),
            *[pltpu.VMEM((model, width), bf)] * 3,
            pltpu.VMEM((1, model), f32),
            dma((8,)),
            pltpu.VMEM((chunks, 2, rows // 2, model), bf),
            pltpu.VMEM((3, width, model), bf),
            pltpu.VMEM((block, block), bf),
            pltpu.VMEM((block, block), bf),
            pltpu.VMEM((2, half, block), bf),
            pltpu.VMEM((half, block), bf),
            pltpu.VMEM((half, block), bf),
            pltpu.VMEM((ZN, half, block), bf),
            pltpu.VMEM((2, XN, half, block), bf),
            pltpu.VMEM((2, XN, half, block), bf),
            pltpu.VMEM((2, XN, block, width), bf),
            pltpu.VMEM((width, block), bf),
            *[pltpu.VMEM((block, block), bf)] * 4,
            pltpu.VMEM((width, block), f32),
            pltpu.VMEM((SUB, block), f32),
            pltpu.VMEM((2, ZN, half, block), bf),
            pltpu.VMEM((2, ZN, 1, block), f32),
            pltpu.VMEM((ZN, 2, half, block), bf),
            pltpu.VMEM((ZN, 2, 1, block), f32),
            pltpu.VMEM((chunks, rows, width), bf),
            pltpu.VMEM((YN, rows, 2 * width), bf),
            pltpu.VMEM((chunks, 2, width // 2, model), bf),
            dma((14,)), dma((chunks, 2)), dma((2,)),
            dma((2, 3)), dma((2, XN)), dma((2, 3)), dma((2, XN)),
            dma((7,)), dma((ZN,)),
            dma((2, ZN)), dma((ZN, 2)), dma((2, ZN)), dma((ZN, 2)),
            dma((7,)), dma((chunks,)), dma((14,)), dma((chunks, 2)),
        ],
        compiler_params=pltpu.CompilerParams(collective_id=0, has_side_effects=True, vmem_limit_bytes=56 * 1024 * 1024),
    )(stop_offset, activations, input_gain[None], query_weight, key_weight, value_weight, output_weight, output_gain[None])


def solution(mesh):
    in_specs = (P(("sp", "tp"), None), P(), P(None, "tp"), P(None, "tp"), P(None, "tp"), P("tp"), P("tp", None), P())
    return jax.shard_map(local, mesh=mesh, in_specs=in_specs, out_specs=P(("sp", "tp"), None), check_vma=False)
```

```python
import jax
import jax.numpy as jnp
from jax import lax
from jax.experimental import pallas as pl
from jax.experimental.pallas import tpu as pltpu
from jax.sharding import PartitionSpec as P

epsilon = 1e-06
SUB = 8
NT = (((1,), (1,)), ((), ()))
MESH = pl.DeviceIdType.MESH
XN, ZN, YN = 4, 8, 4
LAST = ZN - 1
Q_ORDER = (7, 6, 1, 5, 2, 4, 3)
OWN_ORDER = (1, 7, 2, 6, 5, 4, 3)
MATE_ORDER = (6, 2, 5, 3, 4, 7, 1, 0)


def pick(values, index):
    out = jnp.int32(values[0])
    for position, value in enumerate(values[1:], 1):
        out = jnp.where(index == position, jnp.int32(value), out)
    return out


def suffix_products(total):
    row = lax.broadcasted_iota(jnp.int32, total.shape, 0)

    def up(a, k):
        return jnp.where(row < SUB - k, pltpu.roll(a, SUB - k, 0), 1.0)

    y = up(total, 1)
    y = y * up(y, 1)
    y = y * up(y, 2)
    return y * up(y, 4)


def tile_weights(halved, carry, w_ref):
    keys, n = halved.shape
    steps = keys // SUB
    run = jnp.ones((SUB, n), jnp.float32)
    local = []
    for v in range(steps):
        part = run * jnp.tanh(halved[v * SUB : (v + 1) * SUB])
        local.append(run + part)
        run = run - part
    total = run * (2.0**-steps)
    factor = suffix_products(total) * carry
    for u in range(steps // 2):
        pair = jnp.concatenate([local[2 * u] * factor, local[2 * u + 1] * factor], axis=0)
        w_ref[2 * SUB * u : 2 * SUB * (u + 1)] = pair.astype(jnp.bfloat16)
    return jnp.broadcast_to((factor * total)[0:1], (SUB, n))


def layer_kernel(
    off_ref, x_hbm, gain_hbm, wq_hbm, wk_hbm, wv_hbm, wo_hbm, ogain_hbm, out_ref,
    x_ref, gain_ref, wq_ref, wk_ref, wv_ref, ogain_ref, in_sem, xall, wt, pk, pv_, qmine, kmate, vmate, qbuf, kt, vt, kop, qop, wa, wb, wc, wd, acc, carry,
    send_out, send_keep, ret_out, ret_keep, att, att_in, wo_all,
    x_send, x_recv, m_send, k_send, k_recv, v_send, v_recv, q_send, q_recv,
    ro_send, ro_recv, rk_send, rk_recv, a_send, a_recv, w_send, w_recv,
):
    sp, tp = lax.axis_index("sp"), lax.axis_index("tp")
    z, x = lax.div(sp, XN), lax.rem(sp, XN)
    y, c = lax.div(tp, 2), lax.rem(tp, 2)
    mate = LAST - z
    head = lax.div(z, ZN // 2)
    other = 1 - head
    partner = (sp, y * 2 + 1 - c)
    rows, model = x_hbm.shape
    chunks = YN * 2
    block = rows * chunks
    width = wq_hbm.shape[1]
    half = width // 2
    steps = block // SUB
    bf, f32 = jnp.bfloat16, jnp.float32

    def at_tp(o):
        return (sp, o)

    def at_x(o):
        return (z * XN + o, tp)

    def at_z(o):
        return (o * XN + x, tp)

    def copy(src, dst, ss, rs, device):
        return pltpu.make_async_remote_copy(src_ref=src, dst_ref=dst, send_sem=ss, recv_sem=rs, device_id=device, device_id_type=MESH)

    def along_y(d):
        return lax.rem(y + d, YN)

    def along_x(d):
        return lax.rem(x + d, XN)

    barrier = pltpu.get_barrier_semaphore()
    peers = [at_tp(lax.rem(tp + d, chunks)) for d in range(1, chunks)]
    peers += [at_x(along_x(1)), at_x(along_x(XN - 1))]
    peers += [at_z(lax.rem(z + d, ZN)) for d in range(1, ZN)]
    for peer in peers:
        pl.semaphore_signal(barrier, inc=1, device_id=peer, device_id_type=MESH)
    weights_in = [
        pltpu.make_async_copy(src, dst, in_sem.at[n])
        for n, (src, dst) in enumerate(
            (
                (x_hbm, x_ref), (gain_hbm, gain_ref), (wq_hbm, wq_ref), (wk_hbm, wk_ref), (wv_hbm, wv_ref),
                (wo_hbm.at[0 : width // 2], wo_all.at[tp, 0]), (wo_hbm.at[width // 2 :], wo_all.at[tp, 1]), (ogain_hbm, ogain_ref),
            )
        )
    ]
    for piece in weights_in:
        piece.start()
    weights_in[0].wait()
    weights_in[1].wait()
    wide = x_ref[...].astype(f32)
    spread = jnp.mean(wide * wide, axis=-1, keepdims=True)
    xall[tp] = (wide * lax.rsqrt(spread + epsilon) * gain_ref[...]).astype(bf).reshape(xall.shape[1:])
    pl.semaphore_wait(barrier, len(peers))

    def same(d):
        return along_y(d) * 2 + c

    def across(d):
        return along_y(d) * 2 + 1 - c

    class TpGather:
        def __init__(self, buf, send, recv):
            self.buf, self.send, self.recv = buf, send, recv

        def part(self, chunk, h, slot, device):
            piece = self.buf.at[chunk, h]
            return copy(piece, piece, self.send.at[slot], self.recv.at[chunk, h], device)

        def begin(self):
            for slot, (h, device) in enumerate(((0, same(1)), (1, same(3)), (1, same(1)), (0, same(3)))):
                self.part(tp, h, slot, at_tp(device)).start()
            for h in range(2):
                self.part(tp, h, 4 + h, partner).start()

        def take(self, chunk, h, slot):
            self.part(chunk, h, 0, partner).wait_recv()
            if slot is not None:
                self.part(chunk, h, slot, partner).start()

        def relay(self):
            self.take(same(3), 0, 6)
            self.part(same(3), 0, 12, at_tp(same(1))).start()
            self.take(same(1), 1, 7)
            self.part(same(1), 1, 13, at_tp(same(3))).start()
            self.take(same(3), 1, 8)
            self.take(same(1), 0, 9)

        def relay_far(self):
            self.take(same(2), 0, 10)
            self.take(same(2), 1, 11)

        def complete(self):
            for d in (0, 1, 3, 2):
                for h in range(2):
                    self.take(across(d), h, None)

        def drain(self):
            for slot in range(14):
                self.part(tp, 0, slot, partner).wait_send()

    x_gather = TpGather(xall, x_send, x_recv)
    w_gather = TpGather(wo_all, w_send, w_recv)
    x_gather.begin()
    for piece in weights_in[2:]:
        piece.wait()

    row = lax.broadcasted_iota(jnp.int32, (block, block), 0)
    col = lax.broadcasted_iota(jnp.int32, (1, block), 1)
    step_of = lax.div(col, SUB)
    hit = row == lax.rem(col, SUB) * steps + (steps - 1) - step_of
    pk[...] = jnp.where(hit, 1.0, 0.0).astype(bf)
    pv_[...] = jnp.where(hit, jnp.exp2(-(step_of + 1).astype(f32)), 0.0).astype(bf)
    wt[0] = jnp.transpose(wq_ref[...])
    wt[1] = jnp.transpose(wk_ref[...])
    wt[2] = jnp.transpose(wv_ref[...])
    low = lax.broadcasted_iota(jnp.int32, (half, block), 0)
    first = jnp.full((half, block), off_ref[head] * 0.5, f32)
    one = first.astype(bf)
    rest = first - one.astype(f32)
    two = rest.astype(bf)
    three = (rest - two.astype(f32)).astype(bf)
    qop[half:] = jnp.where(low == 0, one, jnp.where(low == 1, two, jnp.where(low == 2, three, jnp.zeros_like(one))))
    ones = jnp.where(low < 3, 1.0, 0.0).astype(bf)

    x_gather.relay()
    x_gather.relay_far()
    x_gather.complete()

    normed = xall[...].reshape(block, model)
    projected = lax.dot_general(wt[...].reshape(3 * width, model), normed, NT, preferred_element_type=f32).astype(bf)
    q_all = projected[0:width] * bf(0.0625)
    k_all = jnp.dot(projected[width : 2 * width], pk[...], preferred_element_type=f32).astype(bf)
    v_all = jnp.dot(projected[2 * width :], pv_[...], preferred_element_type=f32).astype(bf)
    qmine[...] = q_all.reshape(qmine.shape)
    k_two = k_all.reshape(2, half, block)
    v_two = v_all.reshape(2, half, block)
    upper = head == 1
    kt[head, x] = jnp.where(upper, k_two[1], k_two[0])
    vt[head, x] = jnp.where(upper, v_two[1], v_two[0])
    kmate[...] = jnp.where(upper, k_two[0], k_two[1])
    vmate[...] = jnp.where(upper, v_two[0], v_two[1])

    def k_copy(slab, chunk, slot, device):
        return copy(kt.at[slab, chunk], kt.at[slab, chunk], k_send.at[slab, slot], k_recv.at[slab, chunk], device)

    def v_copy(slab, chunk, slot, device):
        return copy(vt.at[slab, chunk], vt.at[slab, chunk], v_send.at[slab, slot], v_recv.at[slab, chunk], device)

    def mate_copies():
        return (
            copy(kmate, kt.at[head, x], m_send.at[0], k_recv.at[head, x], at_z(mate)),
            copy(vmate, vt.at[head, x], m_send.at[1], v_recv.at[head, x], at_z(mate)),
        )

    def spread_keys(slab):
        for slot, d in ((0, 1), (1, XN - 1)):
            k_copy(slab, x, slot, at_x(along_x(d))).start()

    def spread_values(slab):
        for slot, d in ((0, XN - 1), (1, 1)):
            v_copy(slab, x, slot, at_x(along_x(d))).start()

    left, right = along_x(XN - 1), along_x(1)

    def pass_on(slab):
        k_copy(slab, left, 0, partner).wait_recv()
        k_copy(slab, left, 2, at_x(right)).start()
        v_copy(slab, right, 0, partner).wait_recv()
        v_copy(slab, right, 2, at_x(left)).start()

    def beside(slab):
        v_copy(slab, left, 0, partner).wait_recv()
        k_copy(slab, right, 0, partner).wait_recv()

    def opposite(slab):
        far = along_x(2)
        k_copy(slab, far, 0, partner).wait_recv()
        v_copy(slab, far, 0, partner).wait_recv()

    def key_rows(slab, chunk):
        kop[slab, chunk] = jnp.transpose(jnp.concatenate([kt[slab, chunk], ones], axis=0))

    for sent in mate_copies():
        sent.start()
    spread_keys(head)
    spread_values(head)

    def target(d):
        return lax.rem(z + d, ZN)

    def reaches(d):
        return jnp.minimum(target(d), LAST - target(d)) <= z

    def q_copy(d):
        return copy(qmine.at[lax.div(target(d), ZN // 2)], qbuf.at[z], q_send.at[d - 1], q_recv.at[z], at_z(target(d)))

    for d in Q_ORDER:
        @pl.when(reaches(d))
        def _():
            q_copy(d).start()

    w_gather.begin()

    def q_arrived(source):
        copy(qbuf.at[source], qbuf.at[source], q_send.at[0], q_recv.at[source], partner).wait_recv()

    def scores(slab, kb):
        return jnp.dot(kop[slab, kb], qop[...], preferred_element_type=f32)

    def values(slab, kb, w_ref):
        return jnp.dot(vt[slab, kb], w_ref[...], preferred_element_type=f32)

    centre = (z == ZN // 2 - 1) | (z == ZN // 2)

    def joined(source):
        return centre & (source >= ZN // 2)

    def slab_index(slab, source):
        return jnp.where(joined(source), ZN // 2, jnp.where(slab == head, z, mate))

    def out_copy(slab, source):
        index = slab_index(slab, source)
        return (
            copy(send_keep.at[slab, source], ret_keep.at[index, head], rk_send.at[slab, source], rk_recv.at[index, head], at_z(source)),
            copy(send_out.at[slab, source], ret_out.at[index, head], ro_send.at[slab, source], ro_recv.at[index, head], at_z(source)),
        )

    def deliver(slab, source, part, keep):
        acc[0:half] = part
        carry[...] = keep

        @pl.when(joined(source) & (slab == other))
        def _():
            before, kept = send_out[head, source].astype(f32), send_keep[head, source]
            now = acc[0:half]
            first, second = jnp.where(upper, before, now), jnp.where(upper, now, before)
            acc[0:half] = first + jnp.where(upper, kept, carry[0:1]) * second
            carry[0:1] = carry[0:1] * kept

        waits = joined(source) & (slab == head)

        @pl.when((source == z) & jnp.logical_not(waits))
        def _():
            index = slab_index(slab, source)
            ret_out[index, head] = acc[0:half].astype(bf)
            ret_keep[index, head] = carry[0:1]

        @pl.when((source != z) | waits)
        def _():
            send_out[slab, source] = acc[0:half].astype(bf)
            send_keep[slab, source] = carry[0:1]

        @pl.when((source != z) & jnp.logical_not(waits))
        def _():
            for sent in out_copy(slab, source):
                sent.start()

    def full_set(slab, source):
        qop[0:half] = qbuf[source]
        keep = jnp.ones((SUB, block), f32)
        keep = tile_weights(scores(slab, 3), keep, wa)
        keep = tile_weights(scores(slab, 2), keep, wb)
        part = values(slab, 3, wa)
        keep = tile_weights(scores(slab, 1), keep, wc)
        part = part + values(slab, 2, wb)
        keep = tile_weights(scores(slab, 0), keep, wd)
        part = part + values(slab, 1, wc)
        part = part + values(slab, 0, wd)
        deliver(slab, source, part, keep)

    def diagonal_tile(slab):
        halved = scores(slab, x)
        r = lax.broadcasted_iota(jnp.int32, halved.shape, 0)
        query = lax.broadcasted_iota(jnp.int32, halved.shape, 1)
        key = lax.rem(r, SUB) * steps + (steps - 1) - lax.div(r, SUB)
        halved = jnp.where(key < query, halved, -1e9)
        carry[...] = tile_weights(halved, jnp.ones((SUB, block), f32), wa)
        acc[0:half] = values(slab, x, wa)

    def below_diagonal(slab, source):
        def step(i, t):
            kb = x - 1 - i
            carry[...] = tile_weights(scores(slab, kb), carry[...], wa)
            acc[0:half] += values(slab, kb, wa)
            return t

        lax.fori_loop(0, x, step, 0)
        deliver(slab, source, acc[0:half], carry[...])

    qbuf[z] = qmine[head]
    qop[0:half] = qmine[head]
    key_rows(head, x)
    pass_on(head)
    k_copy(other, x, 0, partner).wait_recv()
    spread_keys(other)
    v_copy(other, x, 0, partner).wait_recv()
    spread_values(other)
    beside(head)
    opposite(head)
    diagonal_tile(head)
    for d in range(1, XN):
        key_rows(head, along_x(d))
    w_gather.relay()
    below_diagonal(head, z)

    def job(n, t):
        @pl.when(n == jnp.where(z < 4, 3, 0))
        def _():
            pass_on(other)

        @pl.when(n == 5)
        def _():
            w_gather.relay_far()

        @pl.when(n == LAST)
        def _():
            beside(other)
            opposite(other)
            for d in range(XN):
                key_rows(other, along_x(d))

        mine = n < LAST
        slab = jnp.where(mine, head, other)
        source = jnp.where(mine, z + pick(OWN_ORDER, n), lax.rem(z + pick(MATE_ORDER, n - LAST), ZN))

        @pl.when((source < ZN) & (mine | (source > mate)))
        def _():
            @pl.when(mine | (source < z))
            def _():
                q_arrived(source)

            full_set(slab, source)

        return t

    lax.fori_loop(0, LAST + ZN, job, 0)

    @pl.when(upper)
    def _():
        q_arrived(mate)

    qop[0:half] = qbuf[mate]
    diagonal_tile(other)
    below_diagonal(other, mate)

    acc[...] = jnp.zeros_like(acc)

    def gather(slab, t):
        for h in range(2):
            low_z = jnp.minimum(slab, LAST - slab)
            provider = low_z if h == 0 else LAST - low_z
            held = (slab != ZN // 2 - 1) | (z < ZN // 2)

            @pl.when(held & (provider != z))
            def _():
                copy(ret_out.at[slab, h], ret_out.at[slab, h], ro_send.at[0, 0], ro_recv.at[slab, h], partner).wait_recv()
                copy(ret_keep.at[slab, h], ret_keep.at[slab, h], rk_send.at[0, 0], rk_recv.at[slab, h], partner).wait_recv()

            @pl.when(held)
            def _():
                span = slice(h * half, (h + 1) * half)
                acc[span] = acc[span] * ret_keep[slab, h] + ret_out[slab, h].astype(f32)

        return t

    lax.fori_loop(0, z + 1, gather, 0)
    att[...] = jnp.transpose(acc[...]).astype(bf).reshape(att.shape)

    def lanes(core):
        return pl.ds(pl.multiple_of(core * width, width), width)

    def a_copy(d):
        o = lax.rem(tp + d, chunks)
        return copy(att.at[o], att_in.at[y, :, lanes(c)], a_send.at[d - 1], a_recv.at[tp], at_tp(o))

    for d in range(1, chunks):
        a_copy(d).start()
    att_in[y, :, lanes(c)] = att[tp]
    w_gather.complete()
    total = jnp.zeros((rows, model), f32)
    for d in (0, 1, 3, 2):
        pair = along_y(d)
        for o in (pair * 2 + 1 - c,) if d == 0 else (pair * 2 + c, pair * 2 + 1 - c):
            slot = att_in.at[pair, :, lanes(lax.rem(o, 2))]
            copy(slot, slot, a_send.at[0], a_recv.at[o], partner).wait_recv()
        both = wo_all[pl.ds(pair * 2, 2)].reshape(2 * width, model)
        total = total + jnp.dot(att_in[pair], both, preferred_element_type=f32)
    spread = jnp.mean(total * total, axis=-1, keepdims=True)
    out_ref[...] = (total * lax.rsqrt(spread + epsilon) * ogain_ref[...]).astype(bf)

    x_gather.drain()
    w_gather.drain()
    for sent in mate_copies():
        sent.wait_send()
    for slab in range(2):
        for slot in range(3):
            k_copy(slab, x, slot, partner).wait_send()
            v_copy(slab, x, slot, partner).wait_send()
    for d in Q_ORDER:
        @pl.when(reaches(d))
        def _():
            q_copy(d).wait_send()
    for d in range(1, chunks):
        a_copy(d).wait_send()

    def drained(source, t):
        @pl.when((source > z) & jnp.logical_not(joined(source)))
        def _():
            for sent in out_copy(head, source):
                sent.wait_send()

        @pl.when((source >= mate) & (source != z))
        def _():
            for sent in out_copy(other, source):
                sent.wait_send()

        return t

    lax.fori_loop(0, ZN, drained, 0)


def local(activations, input_gain, query_weight, key_weight, value_weight, stop_offset, output_weight, output_gain):
    rows, model = activations.shape
    width = query_weight.shape[1]
    half = width // 2
    chunks = lax.axis_size("tp")
    block = rows * chunks
    bf, f32, dma = jnp.bfloat16, jnp.float32, pltpu.SemaphoreType.DMA
    vmem = pl.BlockSpec(memory_space=pltpu.VMEM)
    return pl.pallas_call(
        layer_kernel,
        out_shape=jax.ShapeDtypeStruct((rows, model), bf),
        in_specs=[pl.BlockSpec(memory_space=pltpu.SMEM)] + [pl.BlockSpec(memory_space=pl.ANY)] * 7,
        out_specs=vmem,
        scratch_shapes=[
            pltpu.VMEM((rows, model), bf),
            pltpu.VMEM((1, model), f32),
            *[pltpu.VMEM((model, width), bf)] * 3,
            pltpu.VMEM((1, model), f32),
            dma((8,)),
            pltpu.VMEM((chunks, 2, rows // 2, model), bf),
            pltpu.VMEM((3, width, model), bf),
            pltpu.VMEM((block, block), bf),
            pltpu.VMEM((block, block), bf),
            pltpu.VMEM((2, half, block), bf),
            pltpu.VMEM((half, block), bf),
            pltpu.VMEM((half, block), bf),
            pltpu.VMEM((ZN, half, block), bf),
            pltpu.VMEM((2, XN, half, block), bf),
            pltpu.VMEM((2, XN, half, block), bf),
            pltpu.VMEM((2, XN, block, width), bf),
            pltpu.VMEM((width, block), bf),
            *[pltpu.VMEM((block, block), bf)] * 4,
            pltpu.VMEM((width, block), f32),
            pltpu.VMEM((SUB, block), f32),
            pltpu.VMEM((2, ZN, half, block), bf),
            pltpu.VMEM((2, ZN, 1, block), f32),
            pltpu.VMEM((ZN, 2, half, block), bf),
            pltpu.VMEM((ZN, 2, 1, block), f32),
            pltpu.VMEM((chunks, rows, width), bf),
            pltpu.VMEM((YN, rows, 2 * width), bf),
            pltpu.VMEM((chunks, 2, width // 2, model), bf),
            dma((14,)), dma((chunks, 2)), dma((2,)),
            dma((2, 3)), dma((2, XN)), dma((2, 3)), dma((2, XN)),
            dma((7,)), dma((ZN,)),
            dma((2, ZN)), dma((ZN, 2)), dma((2, ZN)), dma((ZN, 2)),
            dma((7,)), dma((chunks,)), dma((14,)), dma((chunks, 2)),
        ],
        compiler_params=pltpu.CompilerParams(collective_id=0, has_side_effects=True, vmem_limit_bytes=56 * 1024 * 1024),
    )(stop_offset, activations, input_gain[None], query_weight, key_weight, value_weight, output_weight, output_gain[None])


def solution(mesh):
    in_specs = (P(("sp", "tp"), None), P(), P(None, "tp"), P(None, "tp"), P(None, "tp"), P("tp"), P("tp", None), P())
    return jax.shard_map(local, mesh=mesh, in_specs=in_specs, out_specs=P(("sp", "tp"), None), check_vma=False)
```

```python
import jax
import jax.numpy as jnp
from jax import lax
from jax.experimental import pallas as pl
from jax.experimental.pallas import tpu as pltpu
from jax.sharding import PartitionSpec as P

epsilon = 1e-06
SUB = 8
NT = (((1,), (1,)), ((), ()))
MESH = pl.DeviceIdType.MESH
XN, ZN, YN = 4, 8, 4
LAST = ZN - 1
Q_ORDER = (7, 6, 1, 5, 2, 4, 3)
OWN_ORDER = (1, 7, 2, 6, 3, 5, 4)
MATE_ORDER = (6, 2, 5, 3, 4, 7, 1, 0)


def pick(values, index):
    out = jnp.int32(values[0])
    for position, value in enumerate(values[1:], 1):
        out = jnp.where(index == position, jnp.int32(value), out)
    return out


def suffix_products(total):
    row = lax.broadcasted_iota(jnp.int32, total.shape, 0)

    def up(a, k):
        return jnp.where(row < SUB - k, pltpu.roll(a, SUB - k, 0), 1.0)

    y = up(total, 1)
    y = y * up(y, 1)
    y = y * up(y, 2)
    return y * up(y, 4)


def tile_weights(halved, carry, w_ref):
    keys, n = halved.shape
    steps = keys // SUB
    run = jnp.ones((SUB, n), jnp.float32)
    local = []
    for v in range(steps):
        part = run * jnp.tanh(halved[v * SUB : (v + 1) * SUB])
        local.append(run + part)
        run = run - part
    total = run * (2.0**-steps)
    factor = suffix_products(total) * carry
    for u in range(steps // 2):
        pair = jnp.concatenate([local[2 * u] * factor, local[2 * u + 1] * factor], axis=0)
        w_ref[2 * SUB * u : 2 * SUB * (u + 1)] = pair.astype(jnp.bfloat16)
    return jnp.broadcast_to((factor * total)[0:1], (SUB, n))


def layer_kernel(
    off_ref, x_hbm, gain_hbm, wq_hbm, wk_hbm, wv_hbm, wo_hbm, ogain_hbm, out_ref,
    x_ref, gain_ref, wq_ref, wk_ref, wv_ref, ogain_ref, in_sem, xall, wt, pk, pv_, qmine, kmate, vmate, qbuf, kt, vt, kop, qop, wa, wb, wc, wd, acc, carry,
    send_out, send_keep, ret_out, ret_keep, att, att_in, wo_all,
    x_send, x_recv, m_send, k_send, k_recv, v_send, v_recv, q_send, q_recv,
    ro_send, ro_recv, rk_send, rk_recv, a_send, a_recv, w_send, w_recv,
):
    sp, tp = lax.axis_index("sp"), lax.axis_index("tp")
    z, x = lax.div(sp, XN), lax.rem(sp, XN)
    y, c = lax.div(tp, 2), lax.rem(tp, 2)
    mate = LAST - z
    head = lax.div(z, ZN // 2)
    other = 1 - head
    partner = (sp, y * 2 + 1 - c)
    rows, model = x_hbm.shape
    chunks = YN * 2
    block = rows * chunks
    width = wq_hbm.shape[1]
    half = width // 2
    steps = block // SUB
    bf, f32 = jnp.bfloat16, jnp.float32

    def at_tp(o):
        return (sp, o)

    def at_x(o):
        return (z * XN + o, tp)

    def at_z(o):
        return (o * XN + x, tp)

    def copy(src, dst, ss, rs, device):
        return pltpu.make_async_remote_copy(src_ref=src, dst_ref=dst, send_sem=ss, recv_sem=rs, device_id=device, device_id_type=MESH)

    def along_y(d):
        return lax.rem(y + d, YN)

    def along_x(d):
        return lax.rem(x + d, XN)

    barrier = pltpu.get_barrier_semaphore()
    peers = [at_tp(lax.rem(tp + d, chunks)) for d in range(1, chunks)]
    peers += [at_x(along_x(1)), at_x(along_x(XN - 1))]
    peers += [at_z(lax.rem(z + d, ZN)) for d in range(1, ZN)]
    for peer in peers:
        pl.semaphore_signal(barrier, inc=1, device_id=peer, device_id_type=MESH)
    weights_in = [
        pltpu.make_async_copy(src, dst, in_sem.at[n])
        for n, (src, dst) in enumerate(
            (
                (x_hbm, x_ref), (gain_hbm, gain_ref), (wq_hbm, wq_ref), (wk_hbm, wk_ref), (wv_hbm, wv_ref),
                (wo_hbm.at[0 : width // 2], wo_all.at[tp, 0]), (wo_hbm.at[width // 2 :], wo_all.at[tp, 1]), (ogain_hbm, ogain_ref),
            )
        )
    ]
    for piece in weights_in:
        piece.start()
    weights_in[0].wait()
    weights_in[1].wait()
    wide = x_ref[...].astype(f32)
    spread = jnp.mean(wide * wide, axis=-1, keepdims=True)
    xall[tp] = (wide * lax.rsqrt(spread + epsilon) * gain_ref[...]).astype(bf).reshape(xall.shape[1:])
    pl.semaphore_wait(barrier, len(peers))

    def same(d):
        return along_y(d) * 2 + c

    def across(d):
        return along_y(d) * 2 + 1 - c

    class TpGather:
        def __init__(self, buf, send, recv):
            self.buf, self.send, self.recv = buf, send, recv

        def part(self, chunk, h, slot, device):
            piece = self.buf.at[chunk, h]
            return copy(piece, piece, self.send.at[slot], self.recv.at[chunk, h], device)

        def begin(self):
            for slot, (h, device) in enumerate(((0, same(1)), (1, same(3)), (1, same(1)), (0, same(3)))):
                self.part(tp, h, slot, at_tp(device)).start()
            for h in range(2):
                self.part(tp, h, 4 + h, partner).start()

        def take(self, chunk, h, slot):
            self.part(chunk, h, 0, partner).wait_recv()
            if slot is not None:
                self.part(chunk, h, slot, partner).start()

        def relay(self):
            self.take(same(3), 0, 6)
            self.part(same(3), 0, 12, at_tp(same(1))).start()
            self.take(same(1), 1, 7)
            self.part(same(1), 1, 13, at_tp(same(3))).start()
            self.take(same(3), 1, 8)
            self.take(same(1), 0, 9)

        def relay_far(self):
            self.take(same(2), 0, 10)
            self.take(same(2), 1, 11)

        def complete(self):
            for d in (0, 1, 3, 2):
                for h in range(2):
                    self.take(across(d), h, None)

        def drain(self):
            for slot in range(14):
                self.part(tp, 0, slot, partner).wait_send()

    x_gather = TpGather(xall, x_send, x_recv)
    w_gather = TpGather(wo_all, w_send, w_recv)
    x_gather.begin()
    for piece in weights_in[2:]:
        piece.wait()

    row = lax.broadcasted_iota(jnp.int32, (block, block), 0)
    col = lax.broadcasted_iota(jnp.int32, (1, block), 1)
    step_of = lax.div(col, SUB)
    hit = row == lax.rem(col, SUB) * steps + (steps - 1) - step_of
    pk[...] = jnp.where(hit, 1.0, 0.0).astype(bf)
    pv_[...] = jnp.where(hit, jnp.exp2(-(step_of + 1).astype(f32)), 0.0).astype(bf)
    wt[0] = jnp.transpose(wq_ref[...])
    wt[1] = jnp.transpose(wk_ref[...])
    wt[2] = jnp.transpose(wv_ref[...])
    low = lax.broadcasted_iota(jnp.int32, (half, block), 0)
    first = jnp.full((half, block), off_ref[head] * 0.5, f32)
    one = first.astype(bf)
    rest = first - one.astype(f32)
    two = rest.astype(bf)
    three = (rest - two.astype(f32)).astype(bf)
    qop[half:] = jnp.where(low == 0, one, jnp.where(low == 1, two, jnp.where(low == 2, three, jnp.zeros_like(one))))
    ones = jnp.where(low < 3, 1.0, 0.0).astype(bf)

    x_gather.relay()
    x_gather.relay_far()
    x_gather.complete()

    normed = xall[...].reshape(block, model)
    projected = lax.dot_general(wt[...].reshape(3 * width, model), normed, NT, preferred_element_type=f32).astype(bf)
    q_all = projected[0:width] * bf(0.0625)
    k_all = jnp.dot(projected[width : 2 * width], pk[...], preferred_element_type=f32).astype(bf)
    v_all = jnp.dot(projected[2 * width :], pv_[...], preferred_element_type=f32).astype(bf)
    qmine[...] = q_all.reshape(qmine.shape)
    k_two = k_all.reshape(2, half, block)
    v_two = v_all.reshape(2, half, block)
    upper = head == 1
    kt[head, x] = jnp.where(upper, k_two[1], k_two[0])
    vt[head, x] = jnp.where(upper, v_two[1], v_two[0])
    kmate[...] = jnp.where(upper, k_two[0], k_two[1])
    vmate[...] = jnp.where(upper, v_two[0], v_two[1])

    def k_copy(slab, chunk, slot, device):
        return copy(kt.at[slab, chunk], kt.at[slab, chunk], k_send.at[slab, slot], k_recv.at[slab, chunk], device)

    def v_copy(slab, chunk, slot, device):
        return copy(vt.at[slab, chunk], vt.at[slab, chunk], v_send.at[slab, slot], v_recv.at[slab, chunk], device)

    def mate_copies():
        return (
            copy(kmate, kt.at[head, x], m_send.at[0], k_recv.at[head, x], at_z(mate)),
            copy(vmate, vt.at[head, x], m_send.at[1], v_recv.at[head, x], at_z(mate)),
        )

    def spread_keys(slab):
        for slot, d in ((0, 1), (1, XN - 1)):
            k_copy(slab, x, slot, at_x(along_x(d))).start()

    def spread_values(slab):
        for slot, d in ((0, XN - 1), (1, 1)):
            v_copy(slab, x, slot, at_x(along_x(d))).start()

    left, right = along_x(XN - 1), along_x(1)

    def pass_on(slab):
        k_copy(slab, left, 0, partner).wait_recv()
        k_copy(slab, left, 2, at_x(right)).start()
        v_copy(slab, right, 0, partner).wait_recv()
        v_copy(slab, right, 2, at_x(left)).start()

    def beside(slab):
        v_copy(slab, left, 0, partner).wait_recv()
        k_copy(slab, right, 0, partner).wait_recv()

    def opposite(slab):
        far = along_x(2)
        k_copy(slab, far, 0, partner).wait_recv()
        v_copy(slab, far, 0, partner).wait_recv()

    def key_rows(slab, chunk):
        kop[slab, chunk] = jnp.transpose(jnp.concatenate([kt[slab, chunk], ones], axis=0))

    for sent in mate_copies():
        sent.start()
    spread_keys(head)
    spread_values(head)

    def target(d):
        return lax.rem(z + d, ZN)

    def reaches(d):
        return jnp.minimum(target(d), LAST - target(d)) <= z

    def q_copy(d):
        return copy(qmine.at[lax.div(target(d), ZN // 2)], qbuf.at[z], q_send.at[d - 1], q_recv.at[z], at_z(target(d)))

    for d in Q_ORDER:
        @pl.when(reaches(d))
        def _():
            q_copy(d).start()

    w_gather.begin()

    def q_arrived(source):
        copy(qbuf.at[source], qbuf.at[source], q_send.at[0], q_recv.at[source], partner).wait_recv()

    def scores(slab, kb):
        return jnp.dot(kop[slab, kb], qop[...], preferred_element_type=f32)

    def values(slab, kb, w_ref):
        return jnp.dot(vt[slab, kb], w_ref[...], preferred_element_type=f32)

    centre = (z == ZN // 2 - 1) | (z == ZN // 2)

    def joined(source):
        return centre & (source >= ZN // 2)

    def slab_index(slab, source):
        return jnp.where(joined(source), ZN // 2, jnp.where(slab == head, z, mate))

    def out_copy(slab, source):
        index = slab_index(slab, source)
        return (
            copy(send_out.at[slab, source], ret_out.at[index, head], ro_send.at[slab, source], ro_recv.at[index, head], at_z(source)),
            copy(send_keep.at[slab, source], ret_keep.at[index, head], rk_send.at[slab, source], rk_recv.at[index, head], at_z(source)),
        )

    def deliver(slab, source, part, keep):
        send_out[slab, source] = part.astype(bf)
        send_keep[slab, source] = keep[0:1]

        @pl.when(joined(source) & (slab == other))
        def _():
            before, now = send_out[head, source].astype(f32), send_out[slab, source].astype(f32)
            kept, keeps = send_keep[head, source], send_keep[slab, source]
            first, second = jnp.where(upper, before, now), jnp.where(upper, now, before)
            send_out[slab, source] = (first + jnp.where(upper, kept, keeps) * second).astype(bf)
            send_keep[slab, source] = keeps * kept

        waits = joined(source) & (slab == head)

        @pl.when((source == z) & jnp.logical_not(waits))
        def _():
            index = slab_index(slab, source)
            ret_out[index, head] = send_out[slab, source]
            ret_keep[index, head] = send_keep[slab, source]

        @pl.when((source != z) & jnp.logical_not(waits))
        def _():
            for sent in out_copy(slab, source):
                sent.start()

    def full_set(slab, source):
        qop[0:half] = qbuf[source]
        keep = jnp.ones((SUB, block), f32)
        keep = tile_weights(scores(slab, 3), keep, wa)
        keep = tile_weights(scores(slab, 2), keep, wb)
        part = values(slab, 3, wa)
        keep = tile_weights(scores(slab, 1), keep, wc)
        part = part + values(slab, 2, wb)
        keep = tile_weights(scores(slab, 0), keep, wd)
        part = part + values(slab, 1, wc)
        part = part + values(slab, 0, wd)
        deliver(slab, source, part, keep)

    def diagonal_tile(slab):
        halved = scores(slab, x)
        r = lax.broadcasted_iota(jnp.int32, halved.shape, 0)
        query = lax.broadcasted_iota(jnp.int32, halved.shape, 1)
        key = lax.rem(r, SUB) * steps + (steps - 1) - lax.div(r, SUB)
        halved = jnp.where(key < query, halved, -1e9)
        carry[...] = tile_weights(halved, jnp.ones((SUB, block), f32), wa)
        acc[0:half] = values(slab, x, wa)

    def below_diagonal(slab, source):
        def step(i, t):
            kb = x - 1 - i
            carry[...] = tile_weights(scores(slab, kb), carry[...], wa)
            acc[0:half] += values(slab, kb, wa)
            return t

        lax.fori_loop(0, x, step, 0)
        deliver(slab, source, acc[0:half], carry[...])

    qbuf[z] = qmine[head]
    qop[0:half] = qmine[head]
    key_rows(head, x)
    pass_on(head)
    k_copy(other, x, 0, partner).wait_recv()
    spread_keys(other)
    v_copy(other, x, 0, partner).wait_recv()
    spread_values(other)
    beside(head)
    opposite(head)
    diagonal_tile(head)
    for d in range(1, XN):
        key_rows(head, along_x(d))
    w_gather.relay()
    below_diagonal(head, z)

    def job(n, t):
        @pl.when(n == 2)
        def _():
            pass_on(other)

        @pl.when(n == 5)
        def _():
            w_gather.relay_far()

        @pl.when(n == LAST)
        def _():
            beside(other)
            opposite(other)
            for d in range(XN):
                key_rows(other, along_x(d))

        mine = n < LAST
        slab = jnp.where(mine, head, other)
        source = jnp.where(mine, z + pick(OWN_ORDER, n), lax.rem(z + pick(MATE_ORDER, n - LAST), ZN))

        @pl.when((source < ZN) & (mine | (source > mate)))
        def _():
            @pl.when(mine | (source < z))
            def _():
                q_arrived(source)

            full_set(slab, source)

        return t

    lax.fori_loop(0, LAST + ZN, job, 0)

    @pl.when(upper)
    def _():
        q_arrived(mate)

    qop[0:half] = qbuf[mate]
    diagonal_tile(other)
    below_diagonal(other, mate)

    acc[...] = jnp.zeros_like(acc)

    def gather(slab, t):
        for h in range(2):
            low_z = jnp.minimum(slab, LAST - slab)
            provider = low_z if h == 0 else LAST - low_z
            held = (slab != ZN // 2 - 1) | (z < ZN // 2)

            @pl.when(held & (provider != z))
            def _():
                copy(ret_out.at[slab, h], ret_out.at[slab, h], ro_send.at[0, 0], ro_recv.at[slab, h], partner).wait_recv()
                copy(ret_keep.at[slab, h], ret_keep.at[slab, h], rk_send.at[0, 0], rk_recv.at[slab, h], partner).wait_recv()

            @pl.when(held)
            def _():
                span = slice(h * half, (h + 1) * half)
                acc[span] = acc[span] * ret_keep[slab, h] + ret_out[slab, h].astype(f32)

        return t

    lax.fori_loop(0, z + 1, gather, 0)
    att[...] = jnp.transpose(acc[...]).astype(bf).reshape(att.shape)

    def lanes(core):
        return pl.ds(pl.multiple_of(core * width, width), width)

    def a_copy(d):
        o = lax.rem(tp + d, chunks)
        return copy(att.at[o], att_in.at[y, :, lanes(c)], a_send.at[d - 1], a_recv.at[tp], at_tp(o))

    for d in range(1, chunks):
        a_copy(d).start()
    att_in[y, :, lanes(c)] = att[tp]
    w_gather.complete()
    total = jnp.zeros((rows, model), f32)
    for d in (0, 1, 3, 2):
        pair = along_y(d)
        for o in (pair * 2 + 1 - c,) if d == 0 else (pair * 2 + c, pair * 2 + 1 - c):
            slot = att_in.at[pair, :, lanes(lax.rem(o, 2))]
            copy(slot, slot, a_send.at[0], a_recv.at[o], partner).wait_recv()
        both = wo_all[pl.ds(pair * 2, 2)].reshape(2 * width, model)
        total = total + jnp.dot(att_in[pair], both, preferred_element_type=f32)
    spread = jnp.mean(total * total, axis=-1, keepdims=True)
    out_ref[...] = (total * lax.rsqrt(spread + epsilon) * ogain_ref[...]).astype(bf)

    x_gather.drain()
    w_gather.drain()
    for sent in mate_copies():
        sent.wait_send()
    for slab in range(2):
        for slot in range(3):
            k_copy(slab, x, slot, partner).wait_send()
            v_copy(slab, x, slot, partner).wait_send()
    for d in Q_ORDER:
        @pl.when(reaches(d))
        def _():
            q_copy(d).wait_send()
    for d in range(1, chunks):
        a_copy(d).wait_send()

    def drained(source, t):
        @pl.when((source > z) & jnp.logical_not(joined(source)))
        def _():
            for sent in out_copy(head, source):
                sent.wait_send()

        @pl.when((source >= mate) & (source != z))
        def _():
            for sent in out_copy(other, source):
                sent.wait_send()

        return t

    lax.fori_loop(0, ZN, drained, 0)


def local(activations, input_gain, query_weight, key_weight, value_weight, stop_offset, output_weight, output_gain):
    rows, model = activations.shape
    width = query_weight.shape[1]
    half = width // 2
    chunks = lax.axis_size("tp")
    block = rows * chunks
    bf, f32, dma = jnp.bfloat16, jnp.float32, pltpu.SemaphoreType.DMA
    vmem = pl.BlockSpec(memory_space=pltpu.VMEM)
    return pl.pallas_call(
        layer_kernel,
        out_shape=jax.ShapeDtypeStruct((rows, model), bf),
        in_specs=[pl.BlockSpec(memory_space=pltpu.SMEM)] + [pl.BlockSpec(memory_space=pl.ANY)] * 7,
        out_specs=vmem,
        scratch_shapes=[
            pltpu.VMEM((rows, model), bf),
            pltpu.VMEM((1, model), f32),
            *[pltpu.VMEM((model, width), bf)] * 3,
            pltpu.VMEM((1, model), f32),
            dma((8,)),
            pltpu.VMEM((chunks, 2, rows // 2, model), bf),
            pltpu.VMEM((3, width, model), bf),
            pltpu.VMEM((block, block), bf),
            pltpu.VMEM((block, block), bf),
            pltpu.VMEM((2, half, block), bf),
            pltpu.VMEM((half, block), bf),
            pltpu.VMEM((half, block), bf),
            pltpu.VMEM((ZN, half, block), bf),
            pltpu.VMEM((2, XN, half, block), bf),
            pltpu.VMEM((2, XN, half, block), bf),
            pltpu.VMEM((2, XN, block, width), bf),
            pltpu.VMEM((width, block), bf),
            *[pltpu.VMEM((block, block), bf)] * 4,
            pltpu.VMEM((width, block), f32),
            pltpu.VMEM((SUB, block), f32),
            pltpu.VMEM((2, ZN, half, block), bf),
            pltpu.VMEM((2, ZN, 1, block), f32),
            pltpu.VMEM((ZN, 2, half, block), bf),
            pltpu.VMEM((ZN, 2, 1, block), f32),
            pltpu.VMEM((chunks, rows, width), bf),
            pltpu.VMEM((YN, rows, 2 * width), bf),
            pltpu.VMEM((chunks, 2, width // 2, model), bf),
            dma((14,)), dma((chunks, 2)), dma((2,)),
            dma((2, 3)), dma((2, XN)), dma((2, 3)), dma((2, XN)),
            dma((7,)), dma((ZN,)),
            dma((2, ZN)), dma((ZN, 2)), dma((2, ZN)), dma((ZN, 2)),
            dma((7,)), dma((chunks,)), dma((14,)), dma((chunks, 2)),
        ],
        compiler_params=pltpu.CompilerParams(collective_id=0, has_side_effects=True, vmem_limit_bytes=56 * 1024 * 1024),
    )(stop_offset, activations, input_gain[None], query_weight, key_weight, value_weight, output_weight, output_gain[None])


def solution(mesh):
    in_specs = (P(("sp", "tp"), None), P(), P(None, "tp"), P(None, "tp"), P(None, "tp"), P("tp"), P("tp", None), P())
    return jax.shard_map(local, mesh=mesh, in_specs=in_specs, out_specs=P(("sp", "tp"), None), check_vma=False)
```

```python
import jax
import jax.numpy as jnp
from jax import lax
from jax.experimental import pallas as pl
from jax.experimental.pallas import tpu as pltpu
from jax.sharding import PartitionSpec as P

epsilon = 1e-06
SUB = 8
NT = (((1,), (1,)), ((), ()))
MESH = pl.DeviceIdType.MESH
XN, ZN, YN = 4, 8, 4
LAST = ZN - 1
Q_ORDER = (7, 6, 1, 5, 2, 4, 3)
OWN_ORDER = (1, 7, 2, 6, 3, 5, 4)
MATE_ORDER = (6, 2, 5, 3, 4, 7, 1, 0)


def pick(values, index):
    out = jnp.int32(values[0])
    for position, value in enumerate(values[1:], 1):
        out = jnp.where(index == position, jnp.int32(value), out)
    return out


def suffix_products(total):
    row = lax.broadcasted_iota(jnp.int32, total.shape, 0)

    def up(a, k):
        return jnp.where(row < SUB - k, pltpu.roll(a, SUB - k, 0), 1.0)

    y = up(total, 1)
    y = y * up(y, 1)
    y = y * up(y, 2)
    return y * up(y, 4)


def tile_weights(halved, carry, w_ref):
    keys, n = halved.shape
    steps = keys // SUB
    run = jnp.ones((SUB, n), jnp.float32)
    local = []
    for v in range(steps):
        part = run * jnp.tanh(halved[v * SUB : (v + 1) * SUB])
        local.append(run + part)
        run = run - part
    total = run * (2.0**-steps)
    factor = suffix_products(total) * carry
    for u in range(steps // 2):
        pair = jnp.concatenate([local[2 * u] * factor, local[2 * u + 1] * factor], axis=0)
        w_ref[2 * SUB * u : 2 * SUB * (u + 1)] = pair.astype(jnp.bfloat16)
    return jnp.broadcast_to((factor * total)[0:1], (SUB, n))


def layer_kernel(
    off_ref, x_hbm, gain_hbm, wq_hbm, wk_hbm, wv_hbm, wo_hbm, ogain_hbm, out_ref,
    x_ref, gain_ref, wq_ref, wk_ref, wv_ref, ogain_ref, in_sem, xall, wt, pk, pv_, qmine, kmate, vmate, qbuf, kt, vt, kop, qop, wa, wb, wc, wd, acc, carry,
    send_out, send_keep, ret_out, ret_keep, att, att_in, wo_all,
    x_send, x_recv, m_send, k_send, k_recv, v_send, v_recv, q_send, q_recv,
    ro_send, ro_recv, rk_send, rk_recv, a_send, a_recv, w_send, w_recv,
):
    sp, tp = lax.axis_index("sp"), lax.axis_index("tp")
    z, x = lax.div(sp, XN), lax.rem(sp, XN)
    y, c = lax.div(tp, 2), lax.rem(tp, 2)
    mate = LAST - z
    head = lax.div(z, ZN // 2)
    other = 1 - head
    partner = (sp, y * 2 + 1 - c)
    rows, model = x_hbm.shape
    chunks = YN * 2
    block = rows * chunks
    width = wq_hbm.shape[1]
    half = width // 2
    steps = block // SUB
    bf, f32 = jnp.bfloat16, jnp.float32

    def at_tp(o):
        return (sp, o)

    def at_x(o):
        return (z * XN + o, tp)

    def at_z(o):
        return (o * XN + x, tp)

    def copy(src, dst, ss, rs, device):
        return pltpu.make_async_remote_copy(src_ref=src, dst_ref=dst, send_sem=ss, recv_sem=rs, device_id=device, device_id_type=MESH)

    def along_y(d):
        return lax.rem(y + d, YN)

    def along_x(d):
        return lax.rem(x + d, XN)

    barrier = pltpu.get_barrier_semaphore()
    peers = [at_tp(lax.rem(tp + d, chunks)) for d in range(1, chunks)]
    peers += [at_x(along_x(1)), at_x(along_x(XN - 1))]
    peers += [at_z(lax.rem(z + d, ZN)) for d in range(1, ZN)]
    for peer in peers:
        pl.semaphore_signal(barrier, inc=1, device_id=peer, device_id_type=MESH)
    weights_in = [
        pltpu.make_async_copy(src, dst, in_sem.at[n])
        for n, (src, dst) in enumerate(
            (
                (x_hbm, x_ref), (gain_hbm, gain_ref), (wq_hbm, wq_ref), (wk_hbm, wk_ref), (wv_hbm, wv_ref),
                (wo_hbm.at[0 : width // 2], wo_all.at[tp, 0]), (wo_hbm.at[width // 2 :], wo_all.at[tp, 1]), (ogain_hbm, ogain_ref),
            )
        )
    ]
    for piece in weights_in:
        piece.start()
    weights_in[0].wait()
    weights_in[1].wait()
    wide = x_ref[...].astype(f32)
    spread = jnp.mean(wide * wide, axis=-1, keepdims=True)
    xall[tp] = (wide * lax.rsqrt(spread + epsilon) * gain_ref[...]).astype(bf).reshape(xall.shape[1:])
    pl.semaphore_wait(barrier, len(peers))

    def same(d):
        return along_y(d) * 2 + c

    def across(d):
        return along_y(d) * 2 + 1 - c

    class TpGather:
        def __init__(self, buf, send, recv):
            self.buf, self.send, self.recv = buf, send, recv

        def part(self, chunk, h, slot, device):
            piece = self.buf.at[chunk, h]
            return copy(piece, piece, self.send.at[slot], self.recv.at[chunk, h], device)

        def begin(self):
            for slot, (h, device) in enumerate(((0, same(1)), (1, same(3)), (1, same(1)), (0, same(3)))):
                self.part(tp, h, slot, at_tp(device)).start()
            for h in range(2):
                self.part(tp, h, 4 + h, partner).start()

        def take(self, chunk, h, slot):
            self.part(chunk, h, 0, partner).wait_recv()
            if slot is not None:
                self.part(chunk, h, slot, partner).start()

        def relay(self):
            self.take(same(3), 0, 6)
            self.part(same(3), 0, 12, at_tp(same(1))).start()
            self.take(same(1), 1, 7)
            self.part(same(1), 1, 13, at_tp(same(3))).start()
            self.take(same(3), 1, 8)
            self.take(same(1), 0, 9)

        def relay_far(self):
            self.take(same(2), 0, 10)
            self.take(same(2), 1, 11)

        def complete(self):
            for d in (0, 1, 3, 2):
                for h in range(2):
                    self.take(across(d), h, None)

        def drain(self):
            for slot in range(14):
                self.part(tp, 0, slot, partner).wait_send()

    x_gather = TpGather(xall, x_send, x_recv)
    w_gather = TpGather(wo_all, w_send, w_recv)
    x_gather.begin()
    for piece in weights_in[2:]:
        piece.wait()

    row = lax.broadcasted_iota(jnp.int32, (block, block), 0)
    col = lax.broadcasted_iota(jnp.int32, (1, block), 1)
    step_of = lax.div(col, SUB)
    hit = row == lax.rem(col, SUB) * steps + (steps - 1) - step_of
    pk[...] = jnp.where(hit, 1.0, 0.0).astype(bf)
    pv_[...] = jnp.where(hit, jnp.exp2(-(step_of + 1).astype(f32)), 0.0).astype(bf)
    wt[0] = jnp.transpose(wq_ref[...])
    wt[1] = jnp.transpose(wk_ref[...])
    wt[2] = jnp.transpose(wv_ref[...])
    low = lax.broadcasted_iota(jnp.int32, (half, block), 0)
    first = jnp.full((half, block), off_ref[head] * 0.5, f32)
    one = first.astype(bf)
    rest = first - one.astype(f32)
    two = rest.astype(bf)
    three = (rest - two.astype(f32)).astype(bf)
    qop[half:] = jnp.where(low == 0, one, jnp.where(low == 1, two, jnp.where(low == 2, three, jnp.zeros_like(one))))
    ones = jnp.where(low < 3, 1.0, 0.0).astype(bf)

    x_gather.relay()
    x_gather.relay_far()
    x_gather.complete()

    normed = xall[...].reshape(block, model)
    projected = lax.dot_general(wt[...].reshape(3 * width, model), normed, NT, preferred_element_type=f32).astype(bf)
    q_all = projected[0:width] * bf(0.0625)
    k_all = jnp.dot(projected[width : 2 * width], pk[...], preferred_element_type=f32).astype(bf)
    v_all = jnp.dot(projected[2 * width :], pv_[...], preferred_element_type=f32).astype(bf)
    qmine[...] = q_all.reshape(qmine.shape)
    k_two = k_all.reshape(2, half, block)
    v_two = v_all.reshape(2, half, block)
    upper = head == 1
    kt[head, x] = jnp.where(upper, k_two[1], k_two[0])
    vt[head, x] = jnp.where(upper, v_two[1], v_two[0])
    kmate[...] = jnp.where(upper, k_two[0], k_two[1])
    vmate[...] = jnp.where(upper, v_two[0], v_two[1])

    def k_copy(slab, chunk, slot, device):
        return copy(kt.at[slab, chunk], kt.at[slab, chunk], k_send.at[slab, slot], k_recv.at[slab, chunk], device)

    def v_copy(slab, chunk, slot, device):
        return copy(vt.at[slab, chunk], vt.at[slab, chunk], v_send.at[slab, slot], v_recv.at[slab, chunk], device)

    def mate_copies():
        return (
            copy(kmate, kt.at[head, x], m_send.at[0], k_recv.at[head, x], at_z(mate)),
            copy(vmate, vt.at[head, x], m_send.at[1], v_recv.at[head, x], at_z(mate)),
        )

    def spread_keys(slab):
        for slot, d in ((0, 1), (1, XN - 1)):
            k_copy(slab, x, slot, at_x(along_x(d))).start()

    def spread_values(slab):
        for slot, d in ((0, XN - 1), (1, 1)):
            v_copy(slab, x, slot, at_x(along_x(d))).start()

    left, right = along_x(XN - 1), along_x(1)

    def pass_on(slab):
        k_copy(slab, left, 0, partner).wait_recv()
        k_copy(slab, left, 2, at_x(right)).start()
        v_copy(slab, right, 0, partner).wait_recv()
        v_copy(slab, right, 2, at_x(left)).start()

    def beside(slab):
        v_copy(slab, left, 0, partner).wait_recv()
        k_copy(slab, right, 0, partner).wait_recv()

    def opposite(slab):
        far = along_x(2)
        k_copy(slab, far, 0, partner).wait_recv()
        v_copy(slab, far, 0, partner).wait_recv()

    def key_rows(slab, chunk):
        kop[slab, chunk] = jnp.transpose(jnp.concatenate([kt[slab, chunk], ones], axis=0))

    for sent in mate_copies():
        sent.start()
    spread_keys(head)
    spread_values(head)

    def target(d):
        return lax.rem(z + d, ZN)

    def reaches(d):
        return jnp.minimum(target(d), LAST - target(d)) <= z

    def q_copy(d):
        return copy(qmine.at[lax.div(target(d), ZN // 2)], qbuf.at[z], q_send.at[d - 1], q_recv.at[z], at_z(target(d)))

    for d in Q_ORDER:
        @pl.when(reaches(d))
        def _():
            q_copy(d).start()

    w_gather.begin()

    def q_arrived(source):
        copy(qbuf.at[source], qbuf.at[source], q_send.at[0], q_recv.at[source], partner).wait_recv()

    def scores(slab, kb):
        return jnp.dot(kop[slab, kb], qop[...], preferred_element_type=f32)

    def values(slab, kb, w_ref):
        return jnp.dot(vt[slab, kb], w_ref[...], preferred_element_type=f32)

    centre = (z == ZN // 2 - 1) | (z == ZN // 2)

    def joined(source):
        return centre & (source >= ZN // 2)

    def slab_index(slab, source):
        return jnp.where(joined(source), ZN // 2, jnp.where(slab == head, z, mate))

    def out_copy(slab, source):
        index = slab_index(slab, source)
        return (
            copy(send_keep.at[slab, source], ret_keep.at[index, head], rk_send.at[slab, source], rk_recv.at[index, head], at_z(source)),
            copy(send_out.at[slab, source], ret_out.at[index, head], ro_send.at[slab, source], ro_recv.at[index, head], at_z(source)),
        )

    def deliver(slab, source, part, keep):
        send_out[slab, source] = part.astype(bf)
        send_keep[slab, source] = keep[0:1]

        @pl.when(joined(source) & (slab == other))
        def _():
            before, now = send_out[head, source].astype(f32), send_out[slab, source].astype(f32)
            kept, keeps = send_keep[head, source], send_keep[slab, source]
            first, second = jnp.where(upper, before, now), jnp.where(upper, now, before)
            send_out[slab, source] = (first + jnp.where(upper, kept, keeps) * second).astype(bf)
            send_keep[slab, source] = keeps * kept

        waits = joined(source) & (slab == head)

        @pl.when((source == z) & jnp.logical_not(waits))
        def _():
            index = slab_index(slab, source)
            ret_out[index, head] = send_out[slab, source]
            ret_keep[index, head] = send_keep[slab, source]

        @pl.when((source != z) & jnp.logical_not(waits))
        def _():
            for sent in out_copy(slab, source):
                sent.start()

    def full_set(slab, source):
        qop[0:half] = qbuf[source]
        keep = jnp.ones((SUB, block), f32)
        keep = tile_weights(scores(slab, 3), keep, wa)
        keep = tile_weights(scores(slab, 2), keep, wb)
        part = values(slab, 3, wa)
        keep = tile_weights(scores(slab, 1), keep, wc)
        part = part + values(slab, 2, wb)
        keep = tile_weights(scores(slab, 0), keep, wd)
        part = part + values(slab, 1, wc)
        part = part + values(slab, 0, wd)
        deliver(slab, source, part, keep)

    def diagonal_tile(slab):
        halved = scores(slab, x)
        r = lax.broadcasted_iota(jnp.int32, halved.shape, 0)
        query = lax.broadcasted_iota(jnp.int32, halved.shape, 1)
        key = lax.rem(r, SUB) * steps + (steps - 1) - lax.div(r, SUB)
        halved = jnp.where(key < query, halved, -1e9)
        carry[...] = tile_weights(halved, jnp.ones((SUB, block), f32), wa)
        acc[0:half] = values(slab, x, wa)

    def below_diagonal(slab, source):
        def step(i, t):
            kb = x - 1 - i
            carry[...] = tile_weights(scores(slab, kb), carry[...], wa)
            acc[0:half] += values(slab, kb, wa)
            return t

        lax.fori_loop(0, x, step, 0)
        deliver(slab, source, acc[0:half], carry[...])

    qbuf[z] = qmine[head]
    qop[0:half] = qmine[head]
    key_rows(head, x)
    pass_on(head)
    k_copy(other, x, 0, partner).wait_recv()
    spread_keys(other)
    v_copy(other, x, 0, partner).wait_recv()
    spread_values(other)
    beside(head)
    opposite(head)
    diagonal_tile(head)
    for d in range(1, XN):
        key_rows(head, along_x(d))
    w_gather.relay()
    below_diagonal(head, z)

    def job(n, t):
        @pl.when(n == 2)
        def _():
            pass_on(other)

        @pl.when(n == 5)
        def _():
            w_gather.relay_far()

        @pl.when(n == LAST)
        def _():
            beside(other)
            opposite(other)
            for d in range(XN):
                key_rows(other, along_x(d))

        mine = n < LAST
        slab = jnp.where(mine, head, other)
        source = jnp.where(mine, z + pick(OWN_ORDER, n), lax.rem(z + pick(MATE_ORDER, n - LAST), ZN))

        @pl.when((source < ZN) & (mine | (source > mate)))
        def _():
            @pl.when(mine | (source < z))
            def _():
                q_arrived(source)

            full_set(slab, source)

        return t

    lax.fori_loop(0, LAST + ZN, job, 0)

    @pl.when(upper)
    def _():
        q_arrived(mate)

    qop[0:half] = qbuf[mate]
    diagonal_tile(other)
    below_diagonal(other, mate)

    acc[...] = jnp.zeros_like(acc)

    def gather(slab, t):
        for h in range(2):
            low_z = jnp.minimum(slab, LAST - slab)
            provider = low_z if h == 0 else LAST - low_z
            held = (slab != ZN // 2 - 1) | (z < ZN // 2)

            @pl.when(held & (provider != z))
            def _():
                copy(ret_out.at[slab, h], ret_out.at[slab, h], ro_send.at[0, 0], ro_recv.at[slab, h], partner).wait_recv()
                copy(ret_keep.at[slab, h], ret_keep.at[slab, h], rk_send.at[0, 0], rk_recv.at[slab, h], partner).wait_recv()

            @pl.when(held)
            def _():
                span = slice(h * half, (h + 1) * half)
                acc[span] = acc[span] * ret_keep[slab, h] + ret_out[slab, h].astype(f32)

        return t

    lax.fori_loop(0, z + 1, gather, 0)
    att[...] = jnp.transpose(acc[...]).astype(bf).reshape(att.shape)

    def lanes(core):
        return pl.ds(pl.multiple_of(core * width, width), width)

    def a_copy(d):
        o = lax.rem(tp + d, chunks)
        return copy(att.at[o], att_in.at[y, :, lanes(c)], a_send.at[d - 1], a_recv.at[tp], at_tp(o))

    for d in range(1, chunks):
        a_copy(d).start()
    att_in[y, :, lanes(c)] = att[tp]
    w_gather.complete()
    total = jnp.zeros((rows, model), f32)
    for d in (0, 1, 3, 2):
        pair = along_y(d)
        for o in (pair * 2 + 1 - c,) if d == 0 else (pair * 2 + c, pair * 2 + 1 - c):
            slot = att_in.at[pair, :, lanes(lax.rem(o, 2))]
            copy(slot, slot, a_send.at[0], a_recv.at[o], partner).wait_recv()
        both = wo_all[pl.ds(pair * 2, 2)].reshape(2 * width, model)
        total = total + jnp.dot(att_in[pair], both, preferred_element_type=f32)
    spread = jnp.mean(total * total, axis=-1, keepdims=True)
    out_ref[...] = (total * lax.rsqrt(spread + epsilon) * ogain_ref[...]).astype(bf)

    x_gather.drain()
    w_gather.drain()
    for sent in mate_copies():
        sent.wait_send()
    for slab in range(2):
        for slot in range(3):
            k_copy(slab, x, slot, partner).wait_send()
            v_copy(slab, x, slot, partner).wait_send()
    for d in Q_ORDER:
        @pl.when(reaches(d))
        def _():
            q_copy(d).wait_send()
    for d in range(1, chunks):
        a_copy(d).wait_send()

    def drained(source, t):
        @pl.when((source > z) & jnp.logical_not(joined(source)))
        def _():
            for sent in out_copy(head, source):
                sent.wait_send()

        @pl.when((source >= mate) & (source != z))
        def _():
            for sent in out_copy(other, source):
                sent.wait_send()

        return t

    lax.fori_loop(0, ZN, drained, 0)


def local(activations, input_gain, query_weight, key_weight, value_weight, stop_offset, output_weight, output_gain):
    rows, model = activations.shape
    width = query_weight.shape[1]
    half = width // 2
    chunks = lax.axis_size("tp")
    block = rows * chunks
    bf, f32, dma = jnp.bfloat16, jnp.float32, pltpu.SemaphoreType.DMA
    vmem = pl.BlockSpec(memory_space=pltpu.VMEM)
    return pl.pallas_call(
        layer_kernel,
        out_shape=jax.ShapeDtypeStruct((rows, model), bf),
        in_specs=[pl.BlockSpec(memory_space=pltpu.SMEM)] + [pl.BlockSpec(memory_space=pl.ANY)] * 7,
        out_specs=vmem,
        scratch_shapes=[
            pltpu.VMEM((rows, model), bf),
            pltpu.VMEM((1, model), f32),
            *[pltpu.VMEM((model, width), bf)] * 3,
            pltpu.VMEM((1, model), f32),
            dma((8,)),
            pltpu.VMEM((chunks, 2, rows // 2, model), bf),
            pltpu.VMEM((3, width, model), bf),
            pltpu.VMEM((block, block), bf),
            pltpu.VMEM((block, block), bf),
            pltpu.VMEM((2, half, block), bf),
            pltpu.VMEM((half, block), bf),
            pltpu.VMEM((half, block), bf),
            pltpu.VMEM((ZN, half, block), bf),
            pltpu.VMEM((2, XN, half, block), bf),
            pltpu.VMEM((2, XN, half, block), bf),
            pltpu.VMEM((2, XN, block, width), bf),
            pltpu.VMEM((width, block), bf),
            *[pltpu.VMEM((block, block), bf)] * 4,
            pltpu.VMEM((width, block), f32),
            pltpu.VMEM((SUB, block), f32),
            pltpu.VMEM((2, ZN, half, block), bf),
            pltpu.VMEM((2, ZN, 1, block), f32),
            pltpu.VMEM((ZN, 2, half, block), bf),
            pltpu.VMEM((ZN, 2, 1, block), f32),
            pltpu.VMEM((chunks, rows, width), bf),
            pltpu.VMEM((YN, rows, 2 * width), bf),
            pltpu.VMEM((chunks, 2, width // 2, model), bf),
            dma((14,)), dma((chunks, 2)), dma((2,)),
            dma((2, 3)), dma((2, XN)), dma((2, 3)), dma((2, XN)),
            dma((7,)), dma((ZN,)),
            dma((2, ZN)), dma((ZN, 2)), dma((2, ZN)), dma((ZN, 2)),
            dma((7,)), dma((chunks,)), dma((14,)), dma((chunks, 2)),
        ],
        compiler_params=pltpu.CompilerParams(collective_id=0, has_side_effects=True, vmem_limit_bytes=56 * 1024 * 1024),
    )(stop_offset, activations, input_gain[None], query_weight, key_weight, value_weight, output_weight, output_gain[None])


def solution(mesh):
    in_specs = (P(("sp", "tp"), None), P(), P(None, "tp"), P(None, "tp"), P(None, "tp"), P("tp"), P("tp", None), P())
    return jax.shard_map(local, mesh=mesh, in_specs=in_specs, out_specs=P(("sp", "tp"), None), check_vma=False)
```
